32 devices in a mesh: sp: 4 (over z), dp: 8 (over y, x, core).
Axes of the slice: x: 2, y: 2, z: 4, core: 2. Of those that a mesh axis runs over, the one named last changes fastest.
Arguments:
- inputs: bfloat16 [8, 544, 2048], P('dp', 'sp'), may hold values from -6 to 6
- query_vectors: bfloat16 [8, 544, 1024], P('dp', 'sp'), may hold values from -6 to 6
- key_vectors: bfloat16 [8, 544, 1024], P('dp', 'sp'), may hold values from -6 to 6
- value_vectors: bfloat16 [8, 544, 1024], P('dp', 'sp'), may hold values from -6 to 6
- cotangent: bfloat16 [8, 544, 1024], P('dp', 'sp'), may hold values from -6 to 6
- gate_prefix: float32 [8, 16, 544], P('dp', 'sp'), may hold values from -544 to 0, as said below
- value_weight: bfloat16 [2048, 1024], P('sp', 'dp'), may hold values from -0.125 to 0.125
Outputs:
- query_grad: bfloat16 [8, 544, 1024], P('dp', 'sp')
- key_grad: bfloat16 [8, 544, 1024], P('dp', 'sp')
- input_grad: bfloat16 [8, 544, 2048], P('dp', 'sp')
- weight_grad: float32 [2048, 1024], P('sp', 'dp')
The draws below stay inside these ranges and needn't reach their ends.
Inputs may be any that keep to these rules, and one draw needn't show every extreme that they name: `gate_prefix`: non-increasing along the positions of each sequence and head.
All inputs are finite; a program needn't handle non-finite values.
Results may differ from the reference program's by a relative error of at most 0.015.
Values may be sent and summed in bfloat16 or wider, within the bound.
A program may use at most 128 MiB of HBM per device.

```python
import jax
import jax.numpy as jnp
from jax import lax

MODEL = 2048
HEADS = 16
HEAD_DIM = 64
TOK_DEV = 136
VALUE_WIDTH = 1024
SEQS = 8
LEN = 544
QBLOCK = 544


def paired_vectors(key):
    folded = jax.random.fold_in(key, 11)
    query_seed, key_seed, spot_seed, sign_seed = jax.random.split(folded, 4)
    shape = (SEQS, LEN, HEADS * HEAD_DIM)
    query_draw = jnp.clip(jax.random.normal(query_seed, shape, jnp.float32), -4.0, 4.0)
    key_draw = jnp.clip(jax.random.normal(key_seed, shape, jnp.float32), -4.0, 4.0)
    return (query_draw, key_draw)


def draw_query_vectors(key, part):
    return paired_vectors(key)[0].astype(jnp.bfloat16)


def draw_key_vectors(key, part):
    return paired_vectors(key)[1].astype(jnp.bfloat16)


def draw_gate_prefix(key, part):
    folded = jax.random.fold_in(key, 23)
    order_seed, fast_seed, slow_seed, step_seed, span_seed = jax.random.split(folded, 5)
    head_order = jax.random.permutation(order_seed, HEADS)
    fast_count = HEADS // 2
    fast_heads = (head_order < fast_count)[None, :, None]
    fast_rate = jax.random.uniform(fast_seed, (SEQS, HEADS, 1), jnp.float32, 0.05, 0.15)
    slow_rate = jax.random.uniform(slow_seed, (SEQS, HEADS, 1), jnp.float32, 0.25, 0.75) / LEN
    step_rate = jnp.where(fast_heads, fast_rate, slow_rate)
    step_factor = jax.random.uniform(step_seed, (SEQS, HEADS, LEN), jnp.float32, 0.5, 1.5)
    span_factor = jnp.exp(jax.random.uniform(span_seed, (SEQS, HEADS, LEN // TOK_DEV), jnp.float32, -0.6931, 0.6931))
    span_factor = jnp.repeat(span_factor, TOK_DEV, axis=2)
    log_steps = -step_rate * step_factor * span_factor
    return jnp.cumsum(log_steps, axis=2)


def steps_of(key, extent, shards, low, largest):
    loudness = 1.0
    for position, shards_of in shards:
        heights = jax.random.uniform(jax.random.fold_in(jax.random.fold_in(key, 6), position), (shards_of,), jnp.float32, low / len(shards), largest / len(shards))
        loudness = loudness * jnp.repeat(jnp.exp(heights), extent[position] // shards_of).reshape((-1,) + (1,) * (len(extent) - 1 - position))
    return loudness


def noise(rng, dims, spread, limit, shards=(), kind=jnp.bfloat16):
    drawn = jax.random.normal(rng, dims, jnp.float32) * spread
    if len(shards) > 0:
        drawn = steps_of(rng, dims, shards, -0.22, 0.18) * drawn
    return jnp.clip(drawn, min=-limit, max=limit).astype(kind)


def setup_inputs(seed: int = 0) -> dict:
    key_of = jax.random.split(jax.random.key(seed), 8)
    return {
        "inputs": noise(key_of[0], (SEQS, LEN, MODEL), 1.0, 6.0, ((0, 8), (1, 4))),
        "query_vectors": draw_query_vectors(jax.random.fold_in(key_of[7], 71), 0),
        "key_vectors": draw_key_vectors(jax.random.fold_in(key_of[7], 71), 0),
        "value_vectors": noise(key_of[3], (SEQS, LEN, VALUE_WIDTH), 1.0, 6.0, ((0, 8), (1, 4))),
        "cotangent": noise(key_of[4], (SEQS, LEN, VALUE_WIDTH), 1.0, 6.0, ((0, 8), (1, 4))),
        "gate_prefix": draw_gate_prefix(jax.random.fold_in(key_of[7], 71), 0),
        "value_weight": noise(key_of[6], (MODEL, VALUE_WIDTH), MODEL ** -0.5, 0.125, ((0, 4), (1, 8))),
    }


def sequence_backward(query_heads, key_heads, value_heads, grad_heads, prefix):
    score_scale = HEAD_DIM ** -0.5
    query_wide = query_heads.astype(jnp.float32)
    key_wide = key_heads.astype(jnp.float32)
    value_wide = value_heads.astype(jnp.float32)
    grad_wide = grad_heads.astype(jnp.float32)
    key_accum = jnp.zeros(key_wide.shape, jnp.float32)
    value_accum = jnp.zeros(key_wide.shape, jnp.float32)
    query_parts = []
    for block_index in range(LEN // QBLOCK):
        first_row = block_index * QBLOCK
        last_row = first_row + QBLOCK
        query_rows = query_wide[first_row:last_row]
        key_rows = key_wide[:last_row]
        grad_rows = grad_wide[first_row:last_row]
        scores = jnp.einsum('qhd,khd->hqk', query_rows, key_rows) * score_scale
        scores = scores + prefix[:, first_row:last_row, None] - prefix[:, None, :last_row]
        causal = jnp.arange(last_row)[None, :] <= (first_row + jnp.arange(QBLOCK))[:, None]
        scores = jnp.where(causal[None], scores, -jnp.inf)
        row_peak = jnp.max(scores, axis=-1, keepdims=True)
        raised_scores = jnp.exp(scores - row_peak)
        softmax_rows = raised_scores / jnp.sum(raised_scores, axis=-1, keepdims=True)
        softmax_low = lax.optimization_barrier(softmax_rows.astype(jnp.bfloat16)).astype(jnp.float32)
        value_accum = value_accum.at[:last_row].add(jnp.einsum('hqk,qhd->khd', softmax_low, grad_rows))
        softmax_grad = jnp.einsum('qhd,khd->hqk', grad_rows, value_wide[:last_row])
        row_term = jnp.sum(softmax_rows * softmax_grad, axis=-1, keepdims=True)
        score_grad = softmax_rows * (softmax_grad - row_term)
        score_low = lax.optimization_barrier(score_grad.astype(jnp.bfloat16)).astype(jnp.float32)
        query_parts.append((jnp.einsum('hqk,khd->qhd', score_low, key_rows) * score_scale).astype(jnp.bfloat16))
        key_accum = key_accum.at[:last_row].add(jnp.einsum('hqk,qhd->khd', score_low, query_rows))
    query_grad = jnp.concatenate(query_parts, axis=0)
    key_grad = (key_accum * score_scale).astype(jnp.bfloat16)
    return query_grad, key_grad, value_accum.astype(jnp.bfloat16)


def reference(inputs, query_vectors, key_vectors, value_vectors, cotangent, gate_prefix, value_weight):
    head_shape = (LEN, HEADS, HEAD_DIM)

    def per_sequence(weight_total, sequence_items):
        seq_inputs, seq_query, seq_key, seq_value, seq_grad, seq_prefix = sequence_items
        query_grad, key_grad, value_grad = sequence_backward(
            seq_query.reshape(head_shape), seq_key.reshape(head_shape),
            seq_value.reshape(head_shape), seq_grad.reshape(head_shape), seq_prefix)
        value_flat = value_grad.reshape(LEN, VALUE_WIDTH)
        input_grad = jnp.dot(value_flat, value_weight.T, preferred_element_type=jnp.float32).astype(jnp.bfloat16)
        weight_total = weight_total + jnp.dot(seq_inputs.T, value_flat, preferred_element_type=jnp.float32)
        return weight_total, (query_grad.reshape(LEN, VALUE_WIDTH), key_grad.reshape(LEN, VALUE_WIDTH), input_grad)

    weight_total, outputs = lax.scan(
        per_sequence, jnp.zeros((MODEL, VALUE_WIDTH), jnp.float32),
        (inputs, query_vectors, key_vectors, value_vectors, cotangent, gate_prefix))
    query_grad, key_grad, input_grad = outputs
    return (query_grad, key_grad, input_grad, weight_total)
```

```python
import functools

import jax
import jax.numpy as jnp
from jax import lax
from jax.experimental import pallas as pl
from jax.experimental.pallas import tpu as pltpu
from jax.sharding import PartitionSpec as P

HEAD_DIM = 64


def attention_backward(query_heads, key_heads, value_heads, grad_heads, prefix):
    length = query_heads.shape[0]
    score_scale = HEAD_DIM ** (-0.5)
    block_count = max(1, length // 512)
    block_rows = length // block_count
    key_accum = jnp.zeros(key_heads.shape, jnp.float32)
    value_accum = jnp.zeros(key_heads.shape, jnp.float32)
    query_parts = []
    for block_index in range(block_count):
        first_row = block_index * block_rows
        last_row = first_row + block_rows
        query_rows = query_heads[first_row:last_row]
        key_rows = key_heads[:last_row]
        grad_rows = grad_heads[first_row:last_row]
        scores = (
            jnp.einsum("qhd,khd->hqk", query_rows, key_rows, preferred_element_type=jnp.float32)
            * score_scale
        )
        scores = scores + prefix[:, first_row:last_row, None] - prefix[:, None, :last_row]
        causal = jnp.arange(last_row)[None, :] <= (first_row + jnp.arange(block_rows))[:, None]
        scores = jnp.where(causal[None], scores, -jnp.inf)
        row_peak = jnp.max(scores, axis=-1, keepdims=True)
        raised_scores = jnp.exp(scores - row_peak)
        softmax_rows = raised_scores / jnp.sum(raised_scores, axis=-1, keepdims=True)
        softmax_low = softmax_rows.astype(jnp.bfloat16)
        value_accum = value_accum.at[:last_row].add(
            jnp.einsum("hqk,qhd->khd", softmax_low, grad_rows, preferred_element_type=jnp.float32)
        )
        softmax_grad = jnp.einsum(
            "qhd,khd->hqk", grad_rows, value_heads[:last_row], preferred_element_type=jnp.float32
        )
        row_term = jnp.sum(softmax_rows * softmax_grad, axis=-1, keepdims=True)
        score_low = (softmax_rows * (softmax_grad - row_term)).astype(jnp.bfloat16)
        query_parts.append(
            (
                jnp.einsum("hqk,khd->qhd", score_low, key_rows, preferred_element_type=jnp.float32)
                * score_scale
            ).astype(jnp.bfloat16)
        )
        key_accum = key_accum.at[:last_row].add(
            jnp.einsum("hqk,qhd->khd", score_low, query_rows, preferred_element_type=jnp.float32)
        )
    query_grad = jnp.concatenate(query_parts, axis=0)
    key_grad = (key_accum * score_scale).astype(jnp.bfloat16)
    return (query_grad, key_grad, value_accum.astype(jnp.bfloat16))


def shards(inputs, query_vectors, key_vectors, value_vectors, cotangent, gate_prefix, value_weight):
    query_seq, key_seq, value_seq, grad_seq, input_cols = (
        lax.all_to_all(query_vectors[0], "sp", split_axis=1, concat_axis=0, tiled=True),
        lax.all_to_all(key_vectors[0], "sp", split_axis=1, concat_axis=0, tiled=True),
        lax.all_to_all(value_vectors[0], "sp", split_axis=1, concat_axis=0, tiled=True),
        lax.all_to_all(cotangent[0], "sp", split_axis=1, concat_axis=0, tiled=True),
        lax.all_to_all(inputs[0], "sp", split_axis=1, concat_axis=0, tiled=True),
    )
    length = query_seq.shape[0]
    local_width = query_seq.shape[1]
    head_shape = (length, local_width // HEAD_DIM, HEAD_DIM)
    query_heads, key_heads, value_heads = attention_backward(
        query_seq.reshape(head_shape),
        key_seq.reshape(head_shape),
        value_seq.reshape(head_shape),
        grad_seq.reshape(head_shape),
        gate_prefix[0],
    )
    query_flat = query_heads.reshape(length, local_width)
    key_flat = key_heads.reshape(length, local_width)
    value_flat = value_heads.reshape(length, local_width)
    value_all = lax.all_gather(value_flat, "sp", axis=1, tiled=True)
    weight_block = lax.all_gather(value_weight, "dp", axis=1, tiled=True)
    weight_rows = lax.psum_scatter(
        lax.dot_general(
            value_all, input_cols, (((0,), (0,)), ((), ())), preferred_element_type=jnp.float32
        ).astype(jnp.bfloat16),
        "dp",
        scatter_dimension=0,
        tiled=True,
    ).astype(jnp.float32)
    weight_grad = weight_rows.T
    query_back, key_back = (
        lax.all_to_all(query_flat, "sp", split_axis=0, concat_axis=1, tiled=True),
        lax.all_to_all(key_flat, "sp", split_axis=0, concat_axis=1, tiled=True),
    )
    column_grad = lax.dot_general(
        value_all, weight_block, (((1,), (1,)), ((), ())), preferred_element_type=jnp.float32
    ).astype(jnp.bfloat16)
    input_grad = lax.all_to_all(column_grad, "sp", split_axis=0, concat_axis=1, tiled=True)
    return (query_back[None], key_back[None], input_grad[None], weight_grad)


LANES = 128
MESH = pl.DeviceIdType.MESH


def one_kernel_fits(sp_count, dp_count, inputs, query, key, value, cotangent, gate, weight):
    rows, width = query.shape[1:]
    model = inputs.shape[2]
    return (
        dp_count == 8
        and width == dp_count * LANES
        and width % (sp_count * LANES) == 0
        and gate.shape[1] * sp_count * HEAD_DIM == width
        and gate.shape[2] == rows * sp_count
        and LANES == 2 * HEAD_DIM
        and rows % 8 == 0
        and model % (sp_count * LANES) == 0
        and model % (2 * LANES) == 0
        and sp_count == 4
        and rows * sp_count <= 1024
        and (dp_count * rows + width) * model <= 3 * 2**21
    )


dot = functools.partial(lax.dot_general, preferred_element_type=jnp.float32)
BY_LANES = (((1,), (1,)), ((), ()))
BY_ROWS = (((0,), (0,)), ((), ()))
PLAIN = (((1,), (0,)), ((), ()))
LOWEST = -1e30


def own_lanes(head, *arrays):
    lane = lax.broadcasted_iota(jnp.int32, arrays[0].shape, 1)
    own = (lane < HEAD_DIM) if head == 0 else (lane >= HEAD_DIM)
    return [jnp.where(own, x, 0.0).astype(jnp.bfloat16) for x in arrays]


def lanes(p):
    return pl.ds(p * LANES if isinstance(p, int) else pl.multiple_of(p * LANES, LANES), LANES)


def padded(columns):
    return -(-columns // LANES) * LANES


def plus(total, term):
    return term if total is None else total + term


def causal(scores, rows, keys_first):
    columns = scores.shape[1]
    start = columns - rows
    low = start // LANES * LANES
    tail = scores[:, low:]
    row = lax.broadcasted_iota(jnp.int32, tail.shape, 0)
    column = lax.broadcasted_iota(jnp.int32, tail.shape, 1) + (low - start)
    kept = ((column >= row) | (column < 0)) if keys_first else (column <= row)
    tail = jnp.where(kept, tail, -jnp.inf)
    return jnp.concatenate([scores[:, :low], tail], axis=1) if low else tail


def kernel(
    n, half, in_hbm, q_hbm, k_hbm, v_hbm, g_hbm, gate_ref, w_hbm,
    qg_ref, kg_ref, ig_ref, wg_ref,
    in_ref, q_ref, k_ref, v_ref, g_ref, w_ref,
    kv_in, qg_in, down_in, down_out, up_in, up_out, down_acc, up_acc,
    vg, vg_seq, x_all, w_all, part, part_in, sum_ref,
    gate_all, gate_pad, gate_t, gate_rev, soft, raised, value_dot,
    peaks, factors, row_terms, stats,
    local_sems, send_sems, recv_sems,
):
    s = lax.axis_index("sp")
    d = lax.axis_index("dp")
    core, x, y = d % 2, (d // 2) % 2, d // 4
    rows, model = in_ref.shape
    last = n - 1
    low, high = pl.ds(0, model // 2), pl.ds(model // 2, model // 2)
    block = model // n
    scale = HEAD_DIM ** (-0.5)
    f32, bf16 = jnp.float32, jnp.bfloat16

    fetched = [
        pltpu.make_async_copy(src, dst, local_sems.at[i])
        for i, (src, dst) in enumerate(
            ((k_hbm, k_ref), (q_hbm, q_ref), (in_hbm, in_ref), (w_hbm, w_ref), (v_hbm, v_ref), (g_hbm, g_ref))
        )
    ]
    for copy in fetched:
        copy.start()

    def near(step):
        return (
            d
            + (step % 2) * (1 - 2 * core)
            + ((step // 2) % 2) * (2 - 4 * x)
            + (step // 4) * (4 - 8 * y)
        )

    partner, x_near, y_near, corner = near(1), near(2), near(4), near(6)

    ids = {}
    used = [0]

    def sem(key, count=1):
        if key not in ids:
            ids[key] = used[0]
            used[0] += count
            assert used[0] <= send_sems.shape[0]
        return ids[key]

    def remote(src, dst, send_id, recv_id, to_sp, to_dp):
        return pltpu.make_async_remote_copy(
            src_ref=src,
            dst_ref=dst,
            send_sem=send_sems.at[send_id],
            recv_sem=recv_sems.at[recv_id],
            device_id={"sp": to_sp, "dp": to_dp},
            device_id_type=MESH,
        )

    def named(name, src, dst, to_sp, to_dp):
        i = sem(name)
        return remote(src, dst, i, i, to_sp, to_dp)

    def up(si, a, b, p):
        src = (k_ref, v_ref)[a].at[:, lanes(p)] if b == si else kv_in.at[a, p, b]
        i = sem(("up", a, b), half) + p
        return remote(src, kv_in.at[a, p, b], i, i, s + 1, d)

    def up_arrive(a, b, p):
        i = sem(("up", a, b), half) + p
        remote(kv_in.at[a, p, b], kv_in.at[a, p, b], i, i, (s + 1) % n, d).wait_recv()

    def down(si, a, b, p):
        src = (q_ref, g_ref)[a].at[:, lanes(half + p)] if b == si else qg_in.at[a, p, last - b]
        i = sem(("down", a, b), half) + p
        return remote(src, qg_in.at[a, p, last - b], i, i, s - 1, d)

    def down_arrive(a, b, p):
        i = sem(("down", a, b), half) + p
        remote(qg_in.at[a, p, last - b], qg_in.at[a, p, last - b], i, i, (s + 1) % n, d).wait_recv()

    def down_sum(c, b, p):
        i = sem(("down sum", c, b), half) + p
        return remote(down_out.at[c, p, b], down_in.at[c, p, b], i, i, (s + n - 1) % n, d)

    def up_sum(j, p):
        i = sem(("up sum", j), half) + p
        return remote(up_out.at[p, j], up_in.at[p, j], i, i, (s + 1) % n, d)

    def gate_copy(sender, to):
        i = sem("gate", n)
        return remote(gate_ref, gate_all.at[sender], i + to, i + sender, to, d)

    def stat_width(a, b):
        return padded(rows * (n - max(a, b)))

    def stat_copy(which, sender, to):
        i = sem(("stat", which), n)
        piece = stats.at[which, sender, :, pl.ds(0, stat_width(sender, to))]
        return remote(piece, piece, i + to, i + sender, to, d)

    def hop(si, b, upward):
        src = w_ref if b == si else w_all.at[d, b]
        i = sem(("hop", upward), n) + b
        return remote(src, w_all.at[d, b], i, i, (s + 1) % n if upward else (s + n - 1) % n, d)

    def vg_copy(p):
        i = sem("vg", 2 * half)
        return remote(vg.at[p], vg_seq.at[d], i + p, i + d, s, p)

    def send_vg(p):
        @pl.when(d != p)
        def _():
            vg_copy(p).start()

        @pl.when(d == p)
        def _():
            vg_seq[p] = vg[p]

    def x_copy(name):
        return {
            "x low": lambda: named(name, in_ref.at[:, low], x_all.at[d, :, low], s, x_near),
            "x high": lambda: named(name, in_ref.at[:, high], x_all.at[d, :, high], s, x_near),
            "y high": lambda: named(name, in_ref.at[:, high], x_all.at[d, :, high], s, y_near),
            "y low": lambda: named(name, in_ref.at[:, low], x_all.at[d, :, low], s, y_near),
            "own": lambda: named(name, in_ref, x_all.at[d], s, partner),
            "on y": lambda: named(name, x_all.at[x_near, :, low], x_all.at[x_near, :, low], s, y_near),
            "on x": lambda: named(name, x_all.at[y_near, :, high], x_all.at[y_near, :, high], s, x_near),
            "x over": lambda: named(name, x_all.at[x_near], x_all.at[x_near], s, partner),
            "y over": lambda: named(name, x_all.at[y_near], x_all.at[y_near], s, partner),
            "corner over": lambda: named(name, x_all.at[corner], x_all.at[corner], s, partner),
        }[name]()

    x_start = ("x low", "y high", "x high", "y low", "own")
    x_rest = ("on y", "on x", "x over", "y over", "corner over")

    def x_middle():
        x_copy("x low").wait_recv()
        x_copy("on y").start()
        x_copy("y high").wait_recv()
        x_copy("on x").start()
        x_copy("x high").wait_recv()
        x_copy("x over").start()
        x_copy("y low").wait_recv()
        x_copy("y over").start()

    def x_last():
        x_copy("on y").wait_recv()
        x_copy("on x").wait_recv()
        x_copy("corner over").start()

    w_lower, w_upper = pl.ds(0, block // 2), pl.ds(block // 2, block // 2)

    def w_copy(name, j, own=False):
        src = w_ref if own else w_all.at[d, j]
        key = ("w", name, j)
        return {
            "x": lambda: named(key, src, w_all.at[d, j], s, x_near),
            "y": lambda: named(key, src, w_all.at[d, j], s, y_near),
            "own": lambda: named(key, src, w_all.at[d, j], s, partner),
            "on y": lambda: named(key, w_all.at[x_near, j, w_lower], w_all.at[x_near, j, w_lower], s, y_near),
            "on x": lambda: named(key, w_all.at[y_near, j, w_upper], w_all.at[y_near, j, w_upper], s, x_near),
            "x over": lambda: named(key, w_all.at[x_near, j], w_all.at[x_near, j], s, partner),
            "y over": lambda: named(key, w_all.at[y_near, j], w_all.at[y_near, j], s, partner),
            "corner over": lambda: named(key, w_all.at[corner, j], w_all.at[corner, j], s, partner),
        }[name]()

    w_names = ("x", "y", "own", "on y", "on x", "x over", "y over", "corner over")

    def w_start(j, own=False):
        for name in ("x", "y", "own"):
            w_copy(name, j, own).start()

    def w_middle(j):
        w_copy("x", j).wait_recv()
        w_copy("on y", j).start()
        w_copy("y", j).wait_recv()
        w_copy("on x", j).start()
        w_copy("x over", j).start()
        w_copy("y over", j).start()

    def w_last(j):
        w_copy("on y", j).wait_recv()
        w_copy("on x", j).wait_recv()
        w_copy("corner over", j).start()

    def wide(buffer, a, p, count):
        return buffer[a, p, :count].astype(f32).reshape(count * rows, LANES)

    def own32(ref, p):
        return ref[:, lanes(p)].astype(f32)

    def gate_column(si, head):
        own = gate_t[rows * si : rows * si + rows]
        lane = lax.broadcasted_iota(jnp.int32, own.shape, 1)
        return jnp.sum(jnp.where(lane == head, own, 0.0), axis=1, keepdims=True)

    def softmax_queries(si, p):
        columns = rows * (si + 1)
        q32, g32 = own32(q_ref, p), own32(g_ref, p)
        keys = wide(kv_in, 0, p, si + 1).astype(bf16)
        total = None
        for h in range(2):
            head = 2 * p + h
            q_own, g_own = own_lanes(h, q32, g32)
            scores = dot(q_own, keys, BY_LANES) * scale
            scores = scores + gate_column(si, head) - gate_pad[pl.ds(head, 1), :columns]
            scores = causal(scores, rows, False)
            peak = jnp.max(scores, axis=1, keepdims=True)
            up_scores = jnp.exp(scores - peak)
            part_soft = up_scores * (1.0 / jnp.sum(up_scores, axis=1, keepdims=True))
            soft[head, :, :columns] = part_soft
            total = plus(total, dot(part_soft.astype(bf16), g_own, BY_ROWS))
        return total

    def gradient_queries(si, p):
        columns = rows * (si + 1)
        q32, g32 = own32(q_ref, p), own32(g_ref, p)
        keys32 = wide(kv_in, 0, p, si + 1)
        values = wide(kv_in, 1, p, si + 1).astype(bf16)
        dq = dk = None
        for h in range(2):
            q_own, g_own = own_lanes(h, q32, g32)
            (k_own,) = own_lanes(h, keys32)
            part_soft = soft[2 * p + h, :, :columns]
            soft_grad = dot(g_own, values, BY_LANES)
            row_term = jnp.sum(part_soft * soft_grad, axis=1, keepdims=True)
            score_low = (part_soft * (soft_grad - row_term)).astype(bf16)
            dq = plus(dq, dot(score_low, k_own, PLAIN))
            dk = plus(dk, dot(score_low, q_own, BY_ROWS))
        qg_ref[:, lanes(p)] = (dq * scale).astype(bf16)
        return dk * scale

    def softmax_keys(si, p):
        columns = rows * (n - si)
        k32 = own32(k_ref, half + p)
        queries = wide(qg_in, 0, p, n - si).astype(bf16)
        for h in range(2):
            row = 2 * p + h
            head = 2 * half + row
            (k_own,) = own_lanes(h, k32)
            scores = dot(k_own, queries, BY_LANES) * scale
            scores = scores + gate_rev[pl.ds(head, 1), :columns] - gate_column(si, head)
            scores = causal(scores, rows, True)
            peak = jnp.max(scores, axis=0, keepdims=True)
            up_scores = jnp.exp(scores - peak)
            raised[row, :, :columns] = up_scores
            peaks[pl.ds(row, 1), :columns] = peak
            stats[0, si, pl.ds(row, 1), :columns] = peak + jnp.log(
                jnp.sum(up_scores, axis=0, keepdims=True)
            )

    def stat_pieces(si, which, empty):
        width = padded(rows * (n - si))
        pieces = []
        for u in range(n):
            held = stat_width(si, u)
            piece = stats[which, u, :, :held]
            lane = lax.broadcasted_iota(jnp.int32, piece.shape, 1)
            piece = jnp.where(lane < rows * (n - u), piece, empty)
            if held < width:
                rest = jnp.full((piece.shape[0], width - held), empty, f32)
                piece = jnp.concatenate([piece, rest], axis=1)
            pieces.append(piece)
        return pieces, width

    def join_peaks(si):
        pieces, width = stat_pieces(si, 0, LOWEST)
        peak = functools.reduce(jnp.maximum, pieces)
        total = sum(jnp.exp(piece - peak) for piece in pieces)
        factors[:, :width] = jnp.exp(peaks[:, :width] - (peak + jnp.log(total)))

    def join_terms(si):
        pieces, width = stat_pieces(si, 1, 0.0)
        row_terms[:, :width] = sum(pieces)

    def value_keys(si, p):
        columns = rows * (n - si)
        g32 = wide(qg_in, 1, p, n - si)
        g_all = g32.astype(bf16)
        v32 = own32(v_ref, half + p)
        total = None
        for h in range(2):
            row = 2 * p + h
            (g_own,) = own_lanes(h, g32)
            (v_own,) = own_lanes(h, v32)
            part_soft = raised[row, :, :columns] * factors[pl.ds(row, 1), :columns]
            raised[row, :, :columns] = part_soft
            total = plus(total, dot(part_soft.astype(bf16), g_own, PLAIN))
            soft_grad = dot(v_own, g_all, BY_LANES)
            value_dot[row, :, :columns] = soft_grad
            stats[1, si, pl.ds(row, 1), :columns] = jnp.sum(part_soft * soft_grad, axis=0, keepdims=True)
        vg[half + p] = total.astype(bf16)
        send_vg(half + p)

    def gradient_keys(si, p):
        columns = rows * (n - si)
        q32 = wide(qg_in, 0, p, n - si)
        k32 = own32(k_ref, half + p)
        dq = dk = None
        for h in range(2):
            row = 2 * p + h
            (q_own,) = own_lanes(h, q32)
            (k_own,) = own_lanes(h, k32)
            term = row_terms[pl.ds(row, 1), :columns]
            score_low = (raised[row, :, :columns] * (value_dot[row, :, :columns] - term)).astype(bf16)
            dk = plus(dk, dot(score_low, q_own, PLAIN))
            dq = plus(dq, dot(score_low, k_own, BY_ROWS))
        kg_ref[:, lanes(half + p)] = (dk * scale).astype(bf16)
        return dq * scale

    def pass_down(si, c, p, total):
        for b in range(si + 1):
            value = total[rows * b : rows * (b + 1)]
            if si < last:
                down_sum(c, b, p).wait_recv()
                value = value + down_in[c, p, b].astype(f32)
            value = value.astype(bf16)
            if b < si:
                down_out[c, p, b] = value
                down_sum(c, b, p).start()
            elif c == 0:
                vg[p] = value
                send_vg(p)
            else:
                kg_ref[:, lanes(p)] = value

    def pass_up(si, p, total):
        for j in range(n - si):
            value = total[rows * j : rows * (j + 1)]
            if si > 0:
                up_sum(j, p).wait_recv()
                value = value + up_in[p, j].astype(f32)
            value = value.astype(bf16)
            if j < last - si:
                up_out[p, j] = value
                up_sum(j, p).start()
            else:
                qg_ref[:, lanes(half + p)] = value

    def each(body):
        def step(p, carry):
            body(p)
            return carry

        lax.fori_loop(0, half, step, 0)

    def relay(si, a, t):
        if t == si + 1 and si < last and a == 0:
            for p in range(half):
                up(si, 1, si, p).start()
            hop(si, si, True).start()
        if t == n - si and si > 0 and a == 0:
            for p in range(half):
                down(si, 1, si, p).start()
            hop(si, si, False).start()
        for p in range(half):
            if si - t >= 0 and si < last:
                up_arrive(a, si - t, p)
                up(si, a, si - t, p).start()
            if si + t <= last and si > 0:
                down_arrive(a, si + t, p)
                down(si, a, si + t, p).start()

    def w_relay(si, t):
        if si - t >= 0:
            hop(si, si - t, True).wait_recv()
            if si < last:
                hop(si, si - t, True).start()
            w_start(si - t)
        if si + t <= last:
            hop(si, si + t, False).wait_recv()
            if si > 0:
                hop(si, si + t, False).start()
            w_start(si + t)

    def w_blocks(si, t):
        return [b for b in (si - t, si + t) if 0 <= b <= last]

    def first(si):
        columns, query_columns = rows * (si + 1), rows * (n - si)
        others = [u for u in range(n) if u != si]
        for p in range(half):
            if si < last:
                up(si, 0, si, p).start()
            if si > 0:
                down(si, 0, si, p).start()
        for u in others:
            gate_copy(si, u).start()
        w_start(si, True)
        for name in x_start:
            x_copy(name).start()

        for p in range(half):
            for a, ref in enumerate((k_ref, v_ref)):
                kv_in[a, p, si] = ref[:, lanes(p)]
            for a, ref in enumerate((q_ref, g_ref)):
                qg_in[a, p, last - si] = ref[:, lanes(half + p)]
        gate_pad[...] = jnp.zeros_like(gate_pad)
        for which in range(2):
            stats[which, si] = jnp.zeros(stats.shape[2:], f32)
        peaks[...] = jnp.zeros_like(peaks)
        held = gate_ref.shape[0]
        length = rows * n
        gate_pad[held * si : held * si + held, :length] = gate_ref[...]
        for u in others:
            gate_copy(u, u).wait_recv()
            gate_pad[held * u : held * u + held, :length] = gate_all[u]
        turned = gate_pad[...].T
        gate_t[...] = turned
        back = [turned[rows * b : rows * (b + 1)] for b in reversed(range(n))]
        gate_rev[...] = jnp.concatenate(back + [turned[length:]], axis=0).T

        for t in range(1, n):
            relay(si, 0, t)

        def queries_step(p):
            if si == last:
                for b in range(si):
                    up_arrive(0, b, p)
            total = softmax_queries(si, p)
            if si == last:
                pass_down(si, 0, p, total)
            else:
                down_acc[0, p, : si + 1] = total.reshape(si + 1, rows, LANES)

        def keys_step(p):
            if si == 0:
                for b in range(1, n):
                    down_arrive(0, b, p)
            softmax_keys(si, p)

        def do_keys():
            each(keys_step)
            for u in others:
                stat_copy(0, si, u).start()

        if 2 * si < n:
            each(queries_step)
            do_keys()
        else:
            do_keys()
            each(queries_step)
        x_all[d] = in_ref[...]
        w_all[d, si] = w_ref[...]
        x_middle()
        for t in range(1, n):
            relay(si, 1, t)
        w_middle(si)

        def value_step(p):
            if si == 0:
                for b in range(1, n):
                    down_arrive(1, b, p)
            value_keys(si, p)

        def do_values():
            for u in others:
                stat_copy(0, u, si).wait_recv()
            join_peaks(si)
            each(value_step)
            for u in others:
                stat_copy(1, si, u).start()

        def value_sums():
            if si < last:
                each(lambda p: pass_down(si, 0, p, down_acc[0, p, : si + 1].reshape(columns, LANES)))

        if 2 * si < n:
            do_values()
            value_sums()
        else:
            value_sums()
            do_values()
        w_last(si)
        w_relay(si, 1)
        x_last()

        def gradient_step(p):
            if si == last:
                for b in range(si):
                    up_arrive(1, b, p)
            total = gradient_queries(si, p)
            if si == last:
                pass_down(si, 1, p, total)
            else:
                down_acc[1, p, : si + 1] = total.reshape(si + 1, rows, LANES)

        each(gradient_step)
        w_relay(si, 2)
        for u in others:
            stat_copy(1, u, si).wait_recv()
        join_terms(si)

        def key_gradient_step(p):
            total = gradient_keys(si, p)
            if si == 0:
                pass_up(si, p, total)
            else:
                up_acc[p, : n - si] = total.reshape(n - si, rows, LANES)

        each(key_gradient_step)
        for j in w_blocks(si, 1):
            w_middle(j)

    def second(si, begin, end):
        for p in range(begin, end):
            if si < last:
                pass_down(si, 1, p, down_acc[1, p, : si + 1].reshape(rows * (si + 1), LANES))
            if si > 0:
                pass_up(si, p, up_acc[p, : n - si].reshape(rows * (n - si), LANES))

    def third(si):
        w_relay(si, 3)
        for j in w_blocks(si, 2):
            w_middle(j)
        for j in w_blocks(si, 1):
            w_last(j)
        for j in w_blocks(si, 3):
            w_middle(j)
        for t in (2, 3):
            for j in w_blocks(si, t):
                w_last(j)

    def finish(si):
        for p in range(half):
            for a in range(2):
                for b in range(si + 1):
                    if si < last:
                        up(si, a, b, p).wait_send()
                for b in range(si, n):
                    if si > 0:
                        down(si, a, b, p).wait_send()
            for c in range(2):
                for b in range(si):
                    down_sum(c, b, p).wait_send()
            for j in range(last - si):
                up_sum(j, p).wait_send()
        for u in range(n):
            if u != si:
                gate_copy(si, u).wait_send()
                for which in range(2):
                    stat_copy(which, si, u).wait_send()
        for b in range(n):
            if b <= si and si < last:
                hop(si, b, True).wait_send()
            if b >= si and si > 0:
                hop(si, b, False).wait_send()

    def by_device(body):
        for si in range(n):
            pl.when(s == si)(functools.partial(body, si))

    barrier = pltpu.get_barrier_semaphore()
    for r in range(1, n):
        pl.semaphore_signal(barrier, inc=1, device_id={"sp": (s + r) % n, "dp": d}, device_id_type=MESH)
    for step in range(1, 8):
        pl.semaphore_signal(barrier, inc=1, device_id={"sp": s, "dp": near(step)}, device_id_type=MESH)
    pl.semaphore_wait(barrier, n - 1 + 7)
    for copy in fetched:
        copy.wait()

    by_device(first)

    for name in ("own", "x over", "y over", "corner over"):
        x_copy(name).wait_recv()
    for i in range(2 * half):
        @pl.when(d != i)
        def _():
            k = sem("vg", 2 * half) + i
            remote(vg_seq.at[i], vg_seq.at[i], k, k, s, partner).wait_recv()

    def weight_part(j):
        columns = pl.ds(pl.multiple_of(j * block, LANES), block)
        total = None
        for i in range(8):
            total = plus(total, dot(vg_seq[i], x_all[i, :, columns], BY_ROWS))
        return total

    def part_copy(j, slot, to):
        return named(("part", slot), part.at[j], part_in.at[slot], to, d)

    mate, across = s + 1 - 2 * (s % 2), (s + 2) % n
    far = (mate + 2) % n
    part[far] = weight_part(far).astype(bf16)
    part_copy(far, 0, mate).start()
    part[mate] = weight_part(mate).astype(bf16)
    part_copy(mate, 1, mate).start()
    sum_ref[0] = weight_part(across)
    sum_ref[1] = weight_part(s)
    by_device(lambda si: second(si, 0, half // 2))
    part_copy(far, 0, mate).wait_recv()
    part[across] = (sum_ref[0] + part_in[0].astype(f32)).astype(bf16)
    part_copy(across, 2, across).start()
    by_device(lambda si: second(si, half // 2, half))
    by_device(third)

    for j in range(n):
        for name in ("own", "x over", "y over", "corner over"):
            w_copy(name, j).wait_recv()
    vg_rows = jnp.concatenate([vg[i] for i in range(8)], axis=1)
    for j in range(n):
        w_rows = jnp.concatenate([w_all[i, j] for i in range(8)], axis=1)
        ig_ref[:, j * block : (j + 1) * block] = dot(vg_rows, w_rows, BY_LANES).astype(bf16)

    by_device(finish)
    for name in x_start + x_rest:
        x_copy(name).wait_send()
    for j in range(n):
        for name in w_names:
            w_copy(name, j).wait_send()
    for p in range(2 * half):
        @pl.when(d != p)
        def _():
            vg_copy(p).wait_send()

    part_copy(mate, 1, mate).wait_recv()
    part_copy(across, 2, across).wait_recv()
    total = sum_ref[1] + part_in[1].astype(f32) + part_in[2].astype(f32)
    wg_ref[...] = total.T
    part_copy(far, 0, mate).wait_send()
    part_copy(mate, 1, mate).wait_send()
    part_copy(across, 2, across).wait_send()


def put_out(*refs):
    sems = refs[-1]
    copies = [pltpu.make_async_copy(refs[i], refs[4 + i], sems.at[i]) for i in range(4)]
    for copy in copies:
        copy.start()
    for copy in copies:
        copy.wait()


def fused(mesh, inputs, query, key, value, cotangent, gate, weight):
    n = mesh.shape["sp"]
    rows, width = query.shape[1:]
    model = inputs.shape[2]
    half = width // LANES // 2
    length = n * rows
    wide = padded(length)
    bf16, f32 = jnp.bfloat16, jnp.float32
    copies = 256
    vmem = pl.BlockSpec(memory_space=pltpu.VMEM)
    hbm = pl.BlockSpec(memory_space=pl.ANY)
    results = (
        jax.ShapeDtypeStruct((rows, width), bf16),
        jax.ShapeDtypeStruct((rows, width), bf16),
        jax.ShapeDtypeStruct((rows, model), bf16),
        jax.ShapeDtypeStruct((model // n, LANES), f32),
    )
    outs = pl.pallas_call(
        functools.partial(kernel, n, half),
        out_shape=tuple(pltpu.VMEM(x.shape, x.dtype) for x in results),
        in_specs=[hbm] * 5 + [vmem, hbm],
        out_specs=(vmem,) * 4,
        scratch_shapes=[
            pltpu.VMEM((rows, model), bf16),
            *[pltpu.VMEM((rows, width), bf16)] * 4,
            pltpu.VMEM((model // n, LANES), bf16),
            *[pltpu.VMEM((2, half, n, rows, LANES), bf16)] * 2,
            *[pltpu.VMEM((2, half, n - 1, rows, LANES), bf16)] * 2,
            *[pltpu.VMEM((half, n - 1, rows, LANES), bf16)] * 2,
            pltpu.VMEM((2, half, n, rows, LANES), f32),
            pltpu.VMEM((half, n, rows, LANES), f32),
            pltpu.VMEM((8, rows, LANES), bf16),
            pltpu.VMEM((8, rows, LANES), bf16),
            pltpu.VMEM((8, rows, model), bf16),
            pltpu.VMEM((8, n, model // n, LANES), bf16),
            pltpu.VMEM((n, LANES, model // n), bf16),
            pltpu.VMEM((3, LANES, model // n), bf16),
            pltpu.VMEM((2, LANES, model // n), f32),
            pltpu.VMEM((n, gate.shape[1], length), f32),
            pltpu.VMEM((LANES, wide), f32),
            pltpu.VMEM((wide, LANES), f32),
            pltpu.VMEM((LANES, wide), f32),
            *[pltpu.VMEM((2 * half, rows, length), f32)] * 3,
            *[pltpu.VMEM((2 * half, wide), f32)] * 3,
            pltpu.VMEM((2, n, 2 * half, wide), f32),
            pltpu.SemaphoreType.DMA((6,)),
            pltpu.SemaphoreType.DMA((copies,)),
            pltpu.SemaphoreType.DMA((copies,)),
        ],
        compiler_params=pltpu.CompilerParams(
            collective_id=0, has_side_effects=True, vmem_limit_bytes=60 * 2**20
        ),
    )(inputs[0], query[0], key[0], value[0], cotangent[0], gate[0], weight)
    query_grad, key_grad, input_grad, weight_grad = pl.pallas_call(
        put_out,
        out_shape=results,
        in_specs=[vmem] * 4,
        out_specs=(hbm,) * 4,
        scratch_shapes=[pltpu.SemaphoreType.DMA((4,))],
        compiler_params=pltpu.CompilerParams(vmem_limit_bytes=2**20),
    )(*(pltpu.with_memory_space_constraint(x, pltpu.VMEM) for x in outs))
    return (query_grad[None], key_grad[None], input_grad[None], weight_grad)


def solution(mesh):
    in_specs = (
        P("dp", "sp", None),
        P("dp", "sp", None),
        P("dp", "sp", None),
        P("dp", "sp", None),
        P("dp", "sp", None),
        P("dp", "sp", None),
        P("sp", "dp"),
    )
    out_specs = (P("dp", "sp", None), P("dp", "sp", None), P("dp", "sp", None), P("sp", "dp"))
    sp_count, dp_count = mesh.shape["sp"], mesh.shape["dp"]

    def per_device(*arrays):
        if one_kernel_fits(sp_count, dp_count, *arrays):
            return fused(mesh, *arrays)
        return shards(*arrays)

    return jax.shard_map(per_device, mesh=mesh, in_specs=in_specs, out_specs=out_specs, check_vma=False)
```

```python
import functools

import jax
import jax.numpy as jnp
from jax import lax
from jax.experimental import pallas as pl
from jax.experimental.pallas import tpu as pltpu
from jax.sharding import PartitionSpec as P

HEAD_DIM = 64


def attention_backward(query_heads, key_heads, value_heads, grad_heads, prefix):
    length = query_heads.shape[0]
    score_scale = HEAD_DIM ** (-0.5)
    block_count = max(1, length // 512)
    block_rows = length // block_count
    key_accum = jnp.zeros(key_heads.shape, jnp.float32)
    value_accum = jnp.zeros(key_heads.shape, jnp.float32)
    query_parts = []
    for block_index in range(block_count):
        first_row = block_index * block_rows
        last_row = first_row + block_rows
        query_rows = query_heads[first_row:last_row]
        key_rows = key_heads[:last_row]
        grad_rows = grad_heads[first_row:last_row]
        scores = (
            jnp.einsum("qhd,khd->hqk", query_rows, key_rows, preferred_element_type=jnp.float32)
            * score_scale
        )
        scores = scores + prefix[:, first_row:last_row, None] - prefix[:, None, :last_row]
        causal = jnp.arange(last_row)[None, :] <= (first_row + jnp.arange(block_rows))[:, None]
        scores = jnp.where(causal[None], scores, -jnp.inf)
        row_peak = jnp.max(scores, axis=-1, keepdims=True)
        raised_scores = jnp.exp(scores - row_peak)
        softmax_rows = raised_scores / jnp.sum(raised_scores, axis=-1, keepdims=True)
        softmax_low = softmax_rows.astype(jnp.bfloat16)
        value_accum = value_accum.at[:last_row].add(
            jnp.einsum("hqk,qhd->khd", softmax_low, grad_rows, preferred_element_type=jnp.float32)
        )
        softmax_grad = jnp.einsum(
            "qhd,khd->hqk", grad_rows, value_heads[:last_row], preferred_element_type=jnp.float32
        )
        row_term = jnp.sum(softmax_rows * softmax_grad, axis=-1, keepdims=True)
        score_low = (softmax_rows * (softmax_grad - row_term)).astype(jnp.bfloat16)
        query_parts.append(
            (
                jnp.einsum("hqk,khd->qhd", score_low, key_rows, preferred_element_type=jnp.float32)
                * score_scale
            ).astype(jnp.bfloat16)
        )
        key_accum = key_accum.at[:last_row].add(
            jnp.einsum("hqk,qhd->khd", score_low, query_rows, preferred_element_type=jnp.float32)
        )
    query_grad = jnp.concatenate(query_parts, axis=0)
    key_grad = (key_accum * score_scale).astype(jnp.bfloat16)
    return (query_grad, key_grad, value_accum.astype(jnp.bfloat16))


def shards(inputs, query_vectors, key_vectors, value_vectors, cotangent, gate_prefix, value_weight):
    query_seq, key_seq, value_seq, grad_seq, input_cols = (
        lax.all_to_all(query_vectors[0], "sp", split_axis=1, concat_axis=0, tiled=True),
        lax.all_to_all(key_vectors[0], "sp", split_axis=1, concat_axis=0, tiled=True),
        lax.all_to_all(value_vectors[0], "sp", split_axis=1, concat_axis=0, tiled=True),
        lax.all_to_all(cotangent[0], "sp", split_axis=1, concat_axis=0, tiled=True),
        lax.all_to_all(inputs[0], "sp", split_axis=1, concat_axis=0, tiled=True),
    )
    length = query_seq.shape[0]
    local_width = query_seq.shape[1]
    head_shape = (length, local_width // HEAD_DIM, HEAD_DIM)
    query_heads, key_heads, value_heads = attention_backward(
        query_seq.reshape(head_shape),
        key_seq.reshape(head_shape),
        value_seq.reshape(head_shape),
        grad_seq.reshape(head_shape),
        gate_prefix[0],
    )
    query_flat = query_heads.reshape(length, local_width)
    key_flat = key_heads.reshape(length, local_width)
    value_flat = value_heads.reshape(length, local_width)
    value_all = lax.all_gather(value_flat, "sp", axis=1, tiled=True)
    weight_block = lax.all_gather(value_weight, "dp", axis=1, tiled=True)
    weight_rows = lax.psum_scatter(
        lax.dot_general(
            value_all, input_cols, (((0,), (0,)), ((), ())), preferred_element_type=jnp.float32
        ).astype(jnp.bfloat16),
        "dp",
        scatter_dimension=0,
        tiled=True,
    ).astype(jnp.float32)
    weight_grad = weight_rows.T
    query_back, key_back = (
        lax.all_to_all(query_flat, "sp", split_axis=0, concat_axis=1, tiled=True),
        lax.all_to_all(key_flat, "sp", split_axis=0, concat_axis=1, tiled=True),
    )
    column_grad = lax.dot_general(
        value_all, weight_block, (((1,), (1,)), ((), ())), preferred_element_type=jnp.float32
    ).astype(jnp.bfloat16)
    input_grad = lax.all_to_all(column_grad, "sp", split_axis=0, concat_axis=1, tiled=True)
    return (query_back[None], key_back[None], input_grad[None], weight_grad)


LANES = 128
MESH = pl.DeviceIdType.MESH


def one_kernel_fits(sp_count, dp_count, inputs, query, key, value, cotangent, gate, weight):
    rows, width = query.shape[1:]
    model = inputs.shape[2]
    return (
        dp_count == 8
        and width == dp_count * LANES
        and width % (sp_count * LANES) == 0
        and gate.shape[1] * sp_count * HEAD_DIM == width
        and gate.shape[2] == rows * sp_count
        and LANES == 2 * HEAD_DIM
        and rows % 8 == 0
        and model % (sp_count * LANES) == 0
        and model % (2 * LANES) == 0
        and sp_count == 4
        and rows * sp_count <= 1024
        and (dp_count * rows + width) * model <= 3 * 2**21
    )


dot = functools.partial(lax.dot_general, preferred_element_type=jnp.float32)
BY_LANES = (((1,), (1,)), ((), ()))
BY_ROWS = (((0,), (0,)), ((), ()))
PLAIN = (((1,), (0,)), ((), ()))
LOWEST = -1e30


def own_lanes(head, *arrays):
    lane = lax.broadcasted_iota(jnp.int32, arrays[0].shape, 1)
    own = (lane < HEAD_DIM) if head == 0 else (lane >= HEAD_DIM)
    return [jnp.where(own, x, 0.0).astype(jnp.bfloat16) for x in arrays]


def lanes(p):
    return pl.ds(p * LANES if isinstance(p, int) else pl.multiple_of(p * LANES, LANES), LANES)


def padded(columns):
    return -(-columns // LANES) * LANES


def plus(total, term):
    return term if total is None else total + term


def causal(scores, rows, keys_first):
    columns = scores.shape[1]
    start = columns - rows
    low = start // LANES * LANES
    tail = scores[:, low:]
    row = lax.broadcasted_iota(jnp.int32, tail.shape, 0)
    column = lax.broadcasted_iota(jnp.int32, tail.shape, 1) + (low - start)
    kept = ((column >= row) | (column < 0)) if keys_first else (column <= row)
    tail = jnp.where(kept, tail, -jnp.inf)
    return jnp.concatenate([scores[:, :low], tail], axis=1) if low else tail


def kernel(
    n, half, in_hbm, q_hbm, k_hbm, v_hbm, g_hbm, gate_ref, w_hbm,
    qg_ref, kg_ref, ig_ref, wg_ref,
    in_ref, q_ref, k_ref, v_ref, g_ref, w_ref,
    kv_in, qg_in, down_in, down_out, up_in, up_out, down_acc, up_acc,
    vg, vg_seq, x_all, w_all, part, part_in, sum_ref,
    gate_all, gate_pad, gate_t, gate_rev, soft, raised, value_dot,
    peaks, factors, row_terms, stats,
    local_sems, send_sems, recv_sems,
):
    s = lax.axis_index("sp")
    d = lax.axis_index("dp")
    core, x, y = d % 2, (d // 2) % 2, d // 4
    rows, model = in_ref.shape
    last = n - 1
    low, high = pl.ds(0, model // 2), pl.ds(model // 2, model // 2)
    block = model // n
    scale = HEAD_DIM ** (-0.5)
    f32, bf16 = jnp.float32, jnp.bfloat16

    fetched = [
        pltpu.make_async_copy(src, dst, local_sems.at[i])
        for i, (src, dst) in enumerate(
            ((k_hbm, k_ref), (q_hbm, q_ref), (in_hbm, in_ref), (w_hbm, w_ref), (v_hbm, v_ref), (g_hbm, g_ref))
        )
    ]
    for copy in fetched:
        copy.start()

    def near(step):
        return (
            d
            + (step % 2) * (1 - 2 * core)
            + ((step // 2) % 2) * (2 - 4 * x)
            + (step // 4) * (4 - 8 * y)
        )

    partner, x_near, y_near, corner = near(1), near(2), near(4), near(6)

    ids = {}
    used = [0]

    def sem(key, count=1):
        if key not in ids:
            ids[key] = used[0]
            used[0] += count
            assert used[0] <= recv_sems.shape[0], (key, used, recv_sems.shape)
        return ids[key]

    sent_ids = {}

    def remote(src, dst, kind, recv_id, to_sp, to_dp):
        send_id = sent_ids.setdefault(kind, len(sent_ids))
        assert send_id < send_sems.shape[0]
        return pltpu.make_async_remote_copy(
            src_ref=src,
            dst_ref=dst,
            send_sem=send_sems.at[send_id],
            recv_sem=recv_sems.at[recv_id],
            device_id={"sp": to_sp, "dp": to_dp},
            device_id_type=MESH,
        )

    def sent(kind, ref):
        remote(ref, ref, kind, 0, s, partner).wait_send()

    def arrived(name, ref):
        remote(ref, ref, "up", sem(name), s, partner).wait_recv()

    def up(si, a, b, p):
        src = (k_ref, v_ref)[a].at[:, lanes(p)] if b == si else kv_in.at[a, p, b]
        i = sem(("up", a, b), half) + p
        return remote(src, kv_in.at[a, p, b], "up", i, s + 1, d)

    def up_arrive(a, b, p):
        i = sem(("up", a, b), half) + p
        remote(kv_in.at[a, p, b], kv_in.at[a, p, b], "up", i, (s + 1) % n, d).wait_recv()

    def down(si, a, b, p):
        src = (q_ref, g_ref)[a].at[:, lanes(half + p)] if b == si else qg_in.at[a, p, last - b]
        i = sem(("down", a, b), half) + p
        return remote(src, qg_in.at[a, p, last - b], "down", i, s - 1, d)

    def down_arrive(a, b, p):
        i = sem(("down", a, b), half) + p
        remote(qg_in.at[a, p, last - b], qg_in.at[a, p, last - b], "down", i, (s + 1) % n, d).wait_recv()

    def down_sum(c, b, p):
        i = sem(("down sum", c, b), half) + p
        return remote(down_out.at[c, p, b], down_in.at[c, p, b], "down sum", i, (s + n - 1) % n, d)

    def up_sum(j, p):
        i = sem(("up sum", j), half) + p
        return remote(up_out.at[p, j], up_in.at[p, j], "up sum", i, (s + 1) % n, d)

    def gate_copy(sender, to):
        return remote(gate_ref, gate_all.at[sender], "gate", sem("gate"), to, d)

    def stat_width(a, b):
        return padded(rows * (n - max(a, b)))

    def stat_copy(which, sender, to):
        i = sem(("stat", which), n)
        piece = stats.at[which, sender, :, pl.ds(0, stat_width(sender, to))]
        return remote(piece, piece, ("stat", which), i + sender, to, d)

    def hop(si, b, upward):
        src = w_ref if b == si else w_all.at[d, b]
        i = sem(("hop", upward), n) + b
        return remote(src, w_all.at[d, b], ("hop", upward), i, (s + 1) % n if upward else (s + n - 1) % n, d)

    def vg_copy(p):
        return remote(vg.at[p], vg_seq.at[d], "vg", sem("vg"), s, p)

    def send_vg(p):
        @pl.when(d != p)
        def _():
            vg_copy(p).start()

        @pl.when(d == p)
        def _():
            vg_seq[p] = vg[p]

    def x_copy(name):
        src, dst, to = {
            "x low": (in_ref.at[:, low], x_all.at[d, :, low], x_near),
            "x high": (in_ref.at[:, high], x_all.at[d, :, high], x_near),
            "y high": (in_ref.at[:, high], x_all.at[d, :, high], y_near),
            "y low": (in_ref.at[:, low], x_all.at[d, :, low], y_near),
            "own": (in_ref, x_all.at[d], partner),
            "on y": (x_all.at[x_near, :, low],) * 2 + (y_near,),
            "on x": (x_all.at[y_near, :, high],) * 2 + (x_near,),
            "x over": (x_all.at[x_near],) * 2 + (partner,),
            "y over": (x_all.at[y_near],) * 2 + (partner,),
            "corner over": (x_all.at[corner],) * 2 + (partner,),
        }[name]
        key = "x on" if name[:2] == "on" else "x over" if name[-4:] == "over" or name == "own" else name
        return remote(src, dst, "x", sem(("x", key)), s, to)

    x_start = ("x low", "y high", "x high", "y low", "own")

    def x_middle():
        x_copy("x low").wait_recv()
        x_copy("on y").start()
        x_copy("y high").wait_recv()
        x_copy("on x").start()

    def x_over():
        x_copy("x high").wait_recv()
        x_copy("x over").start()
        x_copy("y low").wait_recv()
        x_copy("y over").start()

    def x_last():
        arrived(("x", "x on"), x_all.at[corner])
        x_copy("corner over").start()

    w_lower, w_upper = pl.ds(0, block // 2), pl.ds(block // 2, block // 2)

    def w_copy(name, j, own=False):
        first = w_ref if own else w_all.at[d, j]
        src, dst, to = {
            "x": (first, w_all.at[d, j], x_near),
            "y": (first, w_all.at[d, j], y_near),
            "own": (first, w_all.at[d, j], partner),
            "on y": (w_all.at[x_near, j, w_lower],) * 2 + (y_near,),
            "on x": (w_all.at[y_near, j, w_upper],) * 2 + (x_near,),
            "x over": (w_all.at[x_near, j],) * 2 + (partner,),
            "y over": (w_all.at[y_near, j],) * 2 + (partner,),
            "corner over": (w_all.at[corner, j],) * 2 + (partner,),
        }[name]
        key = ("on", j) if name[:2] == "on" else "over" if name[-4:] == "over" or name == "own" else (name, j)
        return remote(src, dst, "w", sem(("w", key)), s, to)

    def w_start(j, own=False):
        for name in ("x", "y", "own"):
            w_copy(name, j, own).start()

    def w_middle(j):
        w_copy("x", j).wait_recv()
        w_copy("on y", j).start()
        w_copy("y", j).wait_recv()
        w_copy("on x", j).start()
        w_copy("x over", j).start()
        w_copy("y over", j).start()

    def w_last(j):
        arrived(("w", ("on", j)), w_all.at[corner, j])
        w_copy("corner over", j).start()

    def wide(buffer, a, p, count):
        return buffer[a, p, :count].astype(f32).reshape(count * rows, LANES)

    def own32(ref, p):
        return ref[:, lanes(p)].astype(f32)

    def gate_column(si, head):
        own = gate_t[rows * si : rows * si + rows]
        lane = lax.broadcasted_iota(jnp.int32, own.shape, 1)
        return jnp.sum(jnp.where(lane == head, own, 0.0), axis=1, keepdims=True)

    def softmax_queries(si, p):
        columns = rows * (si + 1)
        q32, g32 = own32(q_ref, p), own32(g_ref, p)
        keys = wide(kv_in, 0, p, si + 1).astype(bf16)
        total = None
        for h in range(2):
            head = 2 * p + h
            q_own, g_own = own_lanes(h, q32, g32)
            scores = dot(q_own, keys, BY_LANES) * scale
            scores = scores + gate_column(si, head) - gate_pad[pl.ds(head, 1), :columns]
            scores = causal(scores, rows, False)
            peak = jnp.max(scores, axis=1, keepdims=True)
            up_scores = jnp.exp(scores - peak)
            part_soft = up_scores * (1.0 / jnp.sum(up_scores, axis=1, keepdims=True))
            soft[head, :, :columns] = part_soft
            total = plus(total, dot(part_soft.astype(bf16), g_own, BY_ROWS))
        return total

    def gradient_queries(si, p):
        columns = rows * (si + 1)
        q32, g32 = own32(q_ref, p), own32(g_ref, p)
        keys32 = wide(kv_in, 0, p, si + 1)
        values = wide(kv_in, 1, p, si + 1).astype(bf16)
        dq = dk = None
        for h in range(2):
            q_own, g_own = own_lanes(h, q32, g32)
            (k_own,) = own_lanes(h, keys32)
            part_soft = soft[2 * p + h, :, :columns]
            soft_grad = dot(g_own, values, BY_LANES)
            row_term = jnp.sum(part_soft * soft_grad, axis=1, keepdims=True)
            score_low = (part_soft * (soft_grad - row_term)).astype(bf16)
            dq = plus(dq, dot(score_low, k_own, PLAIN))
            dk = plus(dk, dot(score_low, q_own, BY_ROWS))
        qg_ref[:, lanes(p)] = (dq * scale).astype(bf16)
        return dk * scale

    def softmax_keys(si, p):
        columns = rows * (n - si)
        k32 = own32(k_ref, half + p)
        queries = wide(qg_in, 0, p, n - si).astype(bf16)
        for h in range(2):
            row = 2 * p + h
            head = 2 * half + row
            (k_own,) = own_lanes(h, k32)
            scores = dot(k_own, queries, BY_LANES) * scale
            scores = scores + gate_rev[pl.ds(head, 1), :columns] - gate_column(si, head)
            scores = causal(scores, rows, True)
            peak = jnp.max(scores, axis=0, keepdims=True)
            up_scores = jnp.exp(scores - peak)
            raised[row, :, :columns] = up_scores
            peaks[pl.ds(row, 1), :columns] = peak
            stats[0, si, pl.ds(row, 1), :columns] = peak + jnp.log(
                jnp.sum(up_scores, axis=0, keepdims=True)
            )

    def stat_pieces(si, which, empty):
        width = padded(rows * (n - si))
        pieces = []
        for u in range(n):
            held = stat_width(si, u)
            piece = stats[which, u, :, :held]
            lane = lax.broadcasted_iota(jnp.int32, piece.shape, 1)
            piece = jnp.where(lane < rows * (n - u), piece, empty)
            if held < width:
                rest = jnp.full((piece.shape[0], width - held), empty, f32)
                piece = jnp.concatenate([piece, rest], axis=1)
            pieces.append(piece)
        return pieces, width

    def join_peaks(si):
        pieces, width = stat_pieces(si, 0, LOWEST)
        peak = functools.reduce(jnp.maximum, pieces)
        total = sum(jnp.exp(piece - peak) for piece in pieces)
        factors[:, :width] = jnp.exp(peaks[:, :width] - (peak + jnp.log(total)))

    def join_terms(si):
        pieces, width = stat_pieces(si, 1, 0.0)
        row_terms[:, :width] = sum(pieces)

    def value_keys(si, p):
        columns = rows * (n - si)
        g32 = wide(qg_in, 1, p, n - si)
        g_all = g32.astype(bf16)
        v32 = own32(v_ref, half + p)
        total = None
        for h in range(2):
            row = 2 * p + h
            (g_own,) = own_lanes(h, g32)
            (v_own,) = own_lanes(h, v32)
            part_soft = raised[row, :, :columns] * factors[pl.ds(row, 1), :columns]
            raised[row, :, :columns] = part_soft
            total = plus(total, dot(part_soft.astype(bf16), g_own, PLAIN))
            soft_grad = dot(v_own, g_all, BY_LANES)
            value_dot[row, :, :columns] = soft_grad
            stats[1, si, pl.ds(row, 1), :columns] = jnp.sum(part_soft * soft_grad, axis=0, keepdims=True)
        vg[half + p] = total.astype(bf16)
        send_vg(half + p)

    def gradient_keys(si, p):
        columns = rows * (n - si)
        q32 = wide(qg_in, 0, p, n - si)
        k32 = own32(k_ref, half + p)
        dq = dk = None
        for h in range(2):
            row = 2 * p + h
            (q_own,) = own_lanes(h, q32)
            (k_own,) = own_lanes(h, k32)
            term = row_terms[pl.ds(row, 1), :columns]
            score_low = (raised[row, :, :columns] * (value_dot[row, :, :columns] - term)).astype(bf16)
            dk = plus(dk, dot(score_low, q_own, PLAIN))
            dq = plus(dq, dot(score_low, k_own, BY_ROWS))
        kg_ref[:, lanes(half + p)] = (dk * scale).astype(bf16)
        return dq * scale

    def pass_down(si, c, p, total):
        for b in range(si + 1):
            value = total[rows * b : rows * (b + 1)]
            if si < last:
                down_sum(c, b, p).wait_recv()
                value = value + down_in[c, p, b].astype(f32)
            value = value.astype(bf16)
            if b < si:
                down_out[c, p, b] = value
                down_sum(c, b, p).start()
            elif c == 0:
                vg[p] = value
                send_vg(p)
            else:
                kg_ref[:, lanes(p)] = value

    def pass_up(si, p, total):
        for j in range(n - si):
            value = total[rows * j : rows * (j + 1)]
            if si > 0:
                up_sum(j, p).wait_recv()
                value = value + up_in[p, j].astype(f32)
            value = value.astype(bf16)
            if j < last - si:
                up_out[p, j] = value
                up_sum(j, p).start()
            else:
                qg_ref[:, lanes(half + p)] = value

    def each(body, begin=0, end=half):
        def step(p, carry):
            body(p)
            return carry

        lax.fori_loop(begin, end, step, 0)

    def relay_up(si, a, t, p):
        if si - t >= 0 and si < last:
            up_arrive(a, si - t, p)
            up(si, a, si - t, p).start()

    def relay_down(si, a, t, p):
        if si + t <= last and si > 0:
            down_arrive(a, si + t, p)
            down(si, a, si + t, p).start()

    def send_own(si, upward, begin, end):
        for p in range(begin, end):
            (up if upward else down)(si, 1, si, p).start()

    def relay(si, a, t):
        for p in range(half):
            relay_up(si, a, t, p)
            relay_down(si, a, t, p)

    def relay_first(si):
        if si in (0, last):
            return
        upper = 2 * si >= n
        relay(si, 0, 1)
        send_own(si, not upper, 0, half)
        for t in range(2, n):
            relay(si, 0, t)
        send_own(si, upper, 0, half)

    def w_relay_up(si, t):
        if si - t >= 0:
            hop(si, si - t, True).wait_recv()
            if si < last:
                hop(si, si - t, True).start()
            w_start(si - t)

    def w_relay_down(si, t):
        if si + t <= last:
            hop(si, si + t, False).wait_recv()
            if si > 0:
                hop(si, si + t, False).start()
            w_start(si + t)

    def w_relay(si, t):
        w_relay_up(si, t)
        w_relay_down(si, t)

    def w_blocks(si, t):
        return [b for b in (si - t, si + t) if 0 <= b <= last]

    def first(si):
        columns, query_columns = rows * (si + 1), rows * (n - si)
        others = [u for u in range(n) if u != si]
        for p in range(half):
            if si < last:
                up(si, 0, si, p).start()
            if si > 0:
                down(si, 0, si, p).start()
        for u in others:
            gate_copy(si, u).start()
        if si == 0:
            send_own(si, True, 0, half)
            hop(si, si, True).start()
        if si == last:
            send_own(si, False, 0, half)
            hop(si, si, False).start()
        for name in x_start:
            x_copy(name).start()
        w_start(si, True)

        for p in range(half):
            for a, ref in enumerate((k_ref, v_ref)):
                kv_in[a, p, si] = ref[:, lanes(p)]
            for a, ref in enumerate((q_ref, g_ref)):
                qg_in[a, p, last - si] = ref[:, lanes(half + p)]
        relay_first(si)

        gate_pad[...] = jnp.zeros_like(gate_pad)
        for which in range(2):
            stats[which, si] = jnp.zeros(stats.shape[2:], f32)
        peaks[...] = jnp.zeros_like(peaks)
        held = gate_ref.shape[0]
        length = rows * n
        gate_pad[held * si : held * si + held, :length] = gate_ref[...]
        arrived("gate", gate_all.at[:last])
        for u in others:
            gate_pad[held * u : held * u + held, :length] = gate_all[u]
        turned = gate_pad[...].T
        gate_t[...] = turned
        back = [turned[rows * b : rows * (b + 1)] for b in reversed(range(n))]
        gate_rev[...] = jnp.concatenate(back + [turned[length:]], axis=0).T

        def queries_step(p):
            relay_up(si, 1, 1, p)
            if si == last:
                for b in range(si):
                    up_arrive(0, b, p)
            total = softmax_queries(si, p)
            if si == last:
                pass_down(si, 0, p, total)
            else:
                down_acc[0, p, : si + 1] = total.reshape(si + 1, rows, LANES)

        def keys_step(p):
            relay_down(si, 1, 1, p)
            if si == 0:
                for b in range(1, n):
                    down_arrive(0, b, p)
            softmax_keys(si, p)

        def gradient_step(p):
            if si == last:
                for b in range(si):
                    up_arrive(1, b, p)
            total = gradient_queries(si, p)
            if si == last:
                pass_down(si, 1, p, total)
            else:
                down_acc[1, p, : si + 1] = total.reshape(si + 1, rows, LANES)

        def do_keys():
            each(keys_step)
            for u in others:
                stat_copy(0, si, u).start()

        if si == 0:
            each(queries_step)
            each(gradient_step)
            do_keys()
        elif 2 * si < n:
            each(queries_step)
            hop(si, si, True).start()
            do_keys()
        else:
            do_keys()
            each(queries_step)
        x_middle()
        for t in range(2, n):
            relay(si, 1, t)
        if 0 < si < last:
            if 2 * si < n:
                hop(si, si, False).start()
                w_relay_up(si, 1)
            else:
                hop(si, si, True).start()
        x_all[d] = in_ref[...]
        w_all[d, si] = w_ref[...]

        def value_step(p):
            if si == 0:
                for b in range(1, n):
                    down_arrive(1, b, p)
            value_keys(si, p)

        def do_values():
            for u in others:
                stat_copy(0, u, si).wait_recv()
            join_peaks(si)
            each(value_step)
            for u in others:
                stat_copy(1, si, u).start()

        def value_sums(begin=0, end=half):
            each(lambda p: pass_down(si, 0, p, down_acc[0, p, : si + 1].reshape(columns, LANES)), begin, end)

        def key_gradient_step(p):
            total = gradient_keys(si, p)
            if si == 0:
                pass_up(si, p, total)
            else:
                up_acc[p, : n - si] = total.reshape(n - si, rows, LANES)

        def do_key_gradients():
            for u in others:
                stat_copy(1, u, si).wait_recv()
            join_terms(si)
            each(key_gradient_step)

        if si == 0:
            do_values()
            x_over()
            do_key_gradients()
            value_sums()
            x_last()
            w_middle(si)
            w_relay(si, 1)
        elif si == last:
            do_values()
            x_over()
            w_middle(si)
            each(gradient_step)
            x_last()
            w_relay(si, 1)
            do_key_gradients()
            w_relay(si, 2)
        elif 2 * si < n:
            do_values()
            x_over()
            w_middle(si)
            value_sums()
            w_relay_down(si, 1)
            each(gradient_step)
            x_last()
            do_key_gradients()
            w_relay(si, 2)
        else:
            value_sums(0, half // 2)
            do_values()
            value_sums(half // 2, half)
            hop(si, si, False).start()
            w_relay_down(si, 1)
            x_over()
            w_middle(si)
            w_relay_up(si, 1)
            each(gradient_step)
            x_last()
            w_relay(si, 2)
            do_key_gradients()

    def chain_down(si, begin, end):
        if si < last:
            for p in range(begin, end):
                pass_down(si, 1, p, down_acc[1, p, : si + 1].reshape(rows * (si + 1), LANES))

    def chain_up(si, begin, end):
        if si > 0:
            for p in range(begin, end):
                pass_up(si, p, up_acc[p, : n - si].reshape(rows * (n - si), LANES))

    def chain_first(si, begin, end):
        (chain_up if 2 * si < n else chain_down)(si, begin, end)

    def chain_rest(si):
        (chain_down if 2 * si < n else chain_up)(si, 0, half)

    def fourth(si):
        if si == 0:
            w_relay(si, 2)
        w_relay(si, 3)
        for j in w_blocks(si, 1):
            w_middle(j)

    def third(si):
        for j in w_blocks(si, 2):
            w_middle(j)
        for j in w_blocks(si, 3):
            w_middle(j)
        chain_rest(si)
        w_last(si)
        for j in w_blocks(si, 1):
            w_last(j)
        for t in (2, 3):
            for j in w_blocks(si, t):
                w_last(j)

    def finish(si):
        if si < last:
            sent("up", kv_in.at[:, :, : si + 1])
            sent("up sum", up_out.at[:, : last - si])
            sent(("hop", True), w_all.at[0, : si + 1])
        if si > 0:
            sent("down", qg_in.at[:, :, : n - si])
            sent("down sum", down_out.at[:, :, :si])
            sent(("hop", False), w_all.at[0, : n - si])
        width = sum(stat_width(si, u) for u in range(n) if u != si)
        count = next(c for c in range(1, n + 1) if width % (c * LANES) == 0 and width // c <= stats.shape[3])
        for which in range(2):
            sent(("stat", which), stats.at[0, :count, :, : width // count])

    def by_device(body):
        for si in range(n):
            pl.when(s == si)(functools.partial(body, si))

    barrier = pltpu.get_barrier_semaphore()
    for r in range(1, n):
        pl.semaphore_signal(barrier, inc=1, device_id={"sp": (s + r) % n, "dp": d}, device_id_type=MESH)
    for step in range(1, 8):
        pl.semaphore_signal(barrier, inc=1, device_id={"sp": s, "dp": near(step)}, device_id_type=MESH)
    pl.semaphore_wait(barrier, n - 1 + 7)
    for copy in fetched:
        copy.wait()

    by_device(first)

    arrived(("x", "x over"), x_all.at[:4])
    arrived("vg", vg_seq.at[:7])

    def weight_part(j):
        columns = pl.ds(pl.multiple_of(j * block, LANES), block)
        total = None
        for i in range(8):
            total = plus(total, dot(vg_seq[i], x_all[i, :, columns], BY_ROWS))
        return total

    side = s // 2
    mate = s + 1 - 2 * (s % 2)
    outer = (s == 0) | (s == last)
    inner = (s > 0) & (s < last)
    outermost, nearest = (1 - side) * last, 2 - side

    def part_copy(j, slot, to):
        return remote(part.at[j], part_in.at[slot], "part", sem("part", 4) + slot, to, d)

    def give(j, k, slot):
        part[j] = sum_ref[k].astype(bf16)
        part_copy(j, slot, mate).start()

    sum_ref[0] = weight_part(jnp.where(outer, outermost, mate))
    pl.when(outer)(lambda: give(outermost, 0, 0))
    pl.when(inner)(lambda: give(mate, 0, 2))
    sum_ref[1] = weight_part(jnp.where(outer, nearest, outermost))
    pl.when(outer)(lambda: give(nearest, 1, 1))
    sum_ref[2] = weight_part(jnp.where(outer, mate, nearest))
    pl.when(outer)(lambda: give(mate, 2, 2))
    sum_ref[3] = weight_part(s)
    by_device(fourth)
    by_device(lambda si: chain_first(si, 0, half))

    @pl.when(inner)
    def _():
        for k, j in ((0, outermost), (1, nearest)):
            part_copy(j, k, j).wait_recv()
            part[j] = (sum_ref[k + 1] + part_in[k].astype(f32)).astype(bf16)
            part_copy(j, 3, j).start()

    by_device(third)

    arrived(("w", "over"), w_all.at[:4])
    vg_rows = jnp.concatenate([vg[i] for i in range(8)], axis=1)
    for j in range(n):
        w_rows = jnp.concatenate([w_all[i, j] for i in range(8)], axis=1)
        ig_ref[:, j * block : (j + 1) * block] = dot(vg_rows, w_rows, BY_LANES).astype(bf16)

    by_device(finish)
    sent("gate", gate_all.at[:last])
    sent("vg", vg_seq.at[:7])
    sent("x", x_all.at[:7])
    sent("w", w_all.at[:7])

    for slot in (2, 3):
        part_copy(s, slot, mate).wait_recv()
    total = sum_ref[3] + part_in[2].astype(f32) + part_in[3].astype(f32)
    wg_ref[...] = total.T
    sent("part", part.at[:3])


def put_out(*refs):
    sems = refs[-1]
    copies = [pltpu.make_async_copy(refs[i], refs[4 + i], sems.at[i]) for i in range(4)]
    for copy in copies:
        copy.start()
    for copy in copies:
        copy.wait()


def fused(mesh, inputs, query, key, value, cotangent, gate, weight):
    n = mesh.shape["sp"]
    rows, width = query.shape[1:]
    model = inputs.shape[2]
    half = width // LANES // 2
    length = n * rows
    wide = padded(length)
    bf16, f32 = jnp.bfloat16, jnp.float32
    copies = 7 * (n - 1) * half + 7 * n + 13
    vmem = pl.BlockSpec(memory_space=pltpu.VMEM)
    hbm = pl.BlockSpec(memory_space=pl.ANY)
    results = (
        jax.ShapeDtypeStruct((rows, width), bf16),
        jax.ShapeDtypeStruct((rows, width), bf16),
        jax.ShapeDtypeStruct((rows, model), bf16),
        jax.ShapeDtypeStruct((model // n, LANES), f32),
    )
    outs = pl.pallas_call(
        functools.partial(kernel, n, half),
        out_shape=tuple(pltpu.VMEM(x.shape, x.dtype) for x in results),
        in_specs=[hbm] * 5 + [vmem, hbm],
        out_specs=(vmem,) * 4,
        scratch_shapes=[
            pltpu.VMEM((rows, model), bf16),
            *[pltpu.VMEM((rows, width), bf16)] * 4,
            pltpu.VMEM((model // n, LANES), bf16),
            *[pltpu.VMEM((2, half, n, rows, LANES), bf16)] * 2,
            *[pltpu.VMEM((2, half, n - 1, rows, LANES), bf16)] * 2,
            *[pltpu.VMEM((half, n - 1, rows, LANES), bf16)] * 2,
            pltpu.VMEM((2, half, n, rows, LANES), f32),
            pltpu.VMEM((half, n, rows, LANES), f32),
            pltpu.VMEM((8, rows, LANES), bf16),
            pltpu.VMEM((8, rows, LANES), bf16),
            pltpu.VMEM((8, rows, model), bf16),
            pltpu.VMEM((8, n, model // n, LANES), bf16),
            pltpu.VMEM((n, LANES, model // n), bf16),
            pltpu.VMEM((4, LANES, model // n), bf16),
            pltpu.VMEM((4, LANES, model // n), f32),
            pltpu.VMEM((n, gate.shape[1], length), f32),
            pltpu.VMEM((LANES, wide), f32),
            pltpu.VMEM((wide, LANES), f32),
            pltpu.VMEM((LANES, wide), f32),
            *[pltpu.VMEM((2 * half, rows, length), f32)] * 3,
            *[pltpu.VMEM((2 * half, wide), f32)] * 3,
            pltpu.VMEM((2, n, 2 * half, wide), f32),
            pltpu.SemaphoreType.DMA((6,)),
            pltpu.SemaphoreType.DMA((13,)),
            pltpu.SemaphoreType.DMA((copies,)),
        ],
        compiler_params=pltpu.CompilerParams(
            collective_id=0, has_side_effects=True, vmem_limit_bytes=60 * 2**20
        ),
    )(inputs[0], query[0], key[0], value[0], cotangent[0], gate[0], weight)
    query_grad, key_grad, input_grad, weight_grad = pl.pallas_call(
        put_out,
        out_shape=results,
        in_specs=[vmem] * 4,
        out_specs=(hbm,) * 4,
        scratch_shapes=[pltpu.SemaphoreType.DMA((4,))],
        compiler_params=pltpu.CompilerParams(vmem_limit_bytes=2**20),
    )(*(pltpu.with_memory_space_constraint(x, pltpu.VMEM) for x in outs))
    return (query_grad[None], key_grad[None], input_grad[None], weight_grad)


def solution(mesh):
    in_specs = (
        P("dp", "sp", None),
        P("dp", "sp", None),
        P("dp", "sp", None),
        P("dp", "sp", None),
        P("dp", "sp", None),
        P("dp", "sp", None),
        P("sp", "dp"),
    )
    out_specs = (P("dp", "sp", None), P("dp", "sp", None), P("dp", "sp", None), P("sp", "dp"))
    sp_count, dp_count = mesh.shape["sp"], mesh.shape["dp"]

    def per_device(*arrays):
        if one_kernel_fits(sp_count, dp_count, *arrays):
            return fused(mesh, *arrays)
        return shards(*arrays)

    return jax.shard_map(per_device, mesh=mesh, in_specs=in_specs, out_specs=out_specs, check_vma=False)
```

```python
import functools

import jax
import jax.numpy as jnp
from jax import lax
from jax.experimental import pallas as pl
from jax.experimental.pallas import tpu as pltpu
from jax.sharding import PartitionSpec as P

HEAD_DIM = 64


def attention_backward(query_heads, key_heads, value_heads, grad_heads, prefix):
    length = query_heads.shape[0]
    score_scale = HEAD_DIM ** (-0.5)
    block_count = max(1, length // 512)
    block_rows = length // block_count
    key_accum = jnp.zeros(key_heads.shape, jnp.float32)
    value_accum = jnp.zeros(key_heads.shape, jnp.float32)
    query_parts = []
    for block_index in range(block_count):
        first_row = block_index * block_rows
        last_row = first_row + block_rows
        query_rows = query_heads[first_row:last_row]
        key_rows = key_heads[:last_row]
        grad_rows = grad_heads[first_row:last_row]
        scores = (
            jnp.einsum("qhd,khd->hqk", query_rows, key_rows, preferred_element_type=jnp.float32)
            * score_scale
        )
        scores = scores + prefix[:, first_row:last_row, None] - prefix[:, None, :last_row]
        causal = jnp.arange(last_row)[None, :] <= (first_row + jnp.arange(block_rows))[:, None]
        scores = jnp.where(causal[None], scores, -jnp.inf)
        row_peak = jnp.max(scores, axis=-1, keepdims=True)
        raised_scores = jnp.exp(scores - row_peak)
        softmax_rows = raised_scores / jnp.sum(raised_scores, axis=-1, keepdims=True)
        softmax_low = softmax_rows.astype(jnp.bfloat16)
        value_accum = value_accum.at[:last_row].add(
            jnp.einsum("hqk,qhd->khd", softmax_low, grad_rows, preferred_element_type=jnp.float32)
        )
        softmax_grad = jnp.einsum(
            "qhd,khd->hqk", grad_rows, value_heads[:last_row], preferred_element_type=jnp.float32
        )
        row_term = jnp.sum(softmax_rows * softmax_grad, axis=-1, keepdims=True)
        score_low = (softmax_rows * (softmax_grad - row_term)).astype(jnp.bfloat16)
        query_parts.append(
            (
                jnp.einsum("hqk,khd->qhd", score_low, key_rows, preferred_element_type=jnp.float32)
                * score_scale
            ).astype(jnp.bfloat16)
        )
        key_accum = key_accum.at[:last_row].add(
            jnp.einsum("hqk,qhd->khd", score_low, query_rows, preferred_element_type=jnp.float32)
        )
    query_grad = jnp.concatenate(query_parts, axis=0)
    key_grad = (key_accum * score_scale).astype(jnp.bfloat16)
    return (query_grad, key_grad, value_accum.astype(jnp.bfloat16))


def shards(inputs, query_vectors, key_vectors, value_vectors, cotangent, gate_prefix, value_weight):
    query_seq, key_seq, value_seq, grad_seq, input_cols = (
        lax.all_to_all(query_vectors[0], "sp", split_axis=1, concat_axis=0, tiled=True),
        lax.all_to_all(key_vectors[0], "sp", split_axis=1, concat_axis=0, tiled=True),
        lax.all_to_all(value_vectors[0], "sp", split_axis=1, concat_axis=0, tiled=True),
        lax.all_to_all(cotangent[0], "sp", split_axis=1, concat_axis=0, tiled=True),
        lax.all_to_all(inputs[0], "sp", split_axis=1, concat_axis=0, tiled=True),
    )
    length = query_seq.shape[0]
    local_width = query_seq.shape[1]
    head_shape = (length, local_width // HEAD_DIM, HEAD_DIM)
    query_heads, key_heads, value_heads = attention_backward(
        query_seq.reshape(head_shape),
        key_seq.reshape(head_shape),
        value_seq.reshape(head_shape),
        grad_seq.reshape(head_shape),
        gate_prefix[0],
    )
    query_flat = query_heads.reshape(length, local_width)
    key_flat = key_heads.reshape(length, local_width)
    value_flat = value_heads.reshape(length, local_width)
    value_all = lax.all_gather(value_flat, "sp", axis=1, tiled=True)
    weight_block = lax.all_gather(value_weight, "dp", axis=1, tiled=True)
    weight_rows = lax.psum_scatter(
        lax.dot_general(
            value_all, input_cols, (((0,), (0,)), ((), ())), preferred_element_type=jnp.float32
        ).astype(jnp.bfloat16),
        "dp",
        scatter_dimension=0,
        tiled=True,
    ).astype(jnp.float32)
    weight_grad = weight_rows.T
    query_back, key_back = (
        lax.all_to_all(query_flat, "sp", split_axis=0, concat_axis=1, tiled=True),
        lax.all_to_all(key_flat, "sp", split_axis=0, concat_axis=1, tiled=True),
    )
    column_grad = lax.dot_general(
        value_all, weight_block, (((1,), (1,)), ((), ())), preferred_element_type=jnp.float32
    ).astype(jnp.bfloat16)
    input_grad = lax.all_to_all(column_grad, "sp", split_axis=0, concat_axis=1, tiled=True)
    return (query_back[None], key_back[None], input_grad[None], weight_grad)


LANES = 128
MESH = pl.DeviceIdType.MESH


def one_kernel_fits(sp_count, dp_count, inputs, query, key, value, cotangent, gate, weight):
    rows, width = query.shape[1:]
    model = inputs.shape[2]
    return (
        dp_count == 8
        and width == dp_count * LANES
        and width % (sp_count * LANES) == 0
        and gate.shape[1] * sp_count * HEAD_DIM == width
        and gate.shape[2] == rows * sp_count
        and LANES == 2 * HEAD_DIM
        and rows % 8 == 0
        and model % (sp_count * LANES) == 0
        and model % (2 * LANES) == 0
        and sp_count == 4
        and rows * sp_count <= 1024
        and (dp_count * rows + width) * model <= 3 * 2**21
    )


dot = functools.partial(lax.dot_general, preferred_element_type=jnp.float32)
BY_LANES = (((1,), (1,)), ((), ()))
BY_ROWS = (((0,), (0,)), ((), ()))
PLAIN = (((1,), (0,)), ((), ()))
LOWEST = -1e30


def own_lanes(head, *arrays):
    lane = lax.broadcasted_iota(jnp.int32, arrays[0].shape, 1)
    own = (lane < HEAD_DIM) if head == 0 else (lane >= HEAD_DIM)
    return [jnp.where(own, x, 0.0).astype(jnp.bfloat16) for x in arrays]


def lanes(p):
    return pl.ds(p * LANES if isinstance(p, int) else pl.multiple_of(p * LANES, LANES), LANES)


def padded(columns):
    return -(-columns // LANES) * LANES


def plus(total, term):
    return term if total is None else total + term


def causal(scores, rows, keys_first):
    columns = scores.shape[1]
    start = columns - rows
    low = start // LANES * LANES
    tail = scores[:, low:]
    row = lax.broadcasted_iota(jnp.int32, tail.shape, 0)
    column = lax.broadcasted_iota(jnp.int32, tail.shape, 1) + (low - start)
    kept = ((column >= row) | (column < 0)) if keys_first else (column <= row)
    tail = jnp.where(kept, tail, -jnp.inf)
    return jnp.concatenate([scores[:, :low], tail], axis=1) if low else tail


def kernel(
    n, half, in_hbm, q_hbm, k_hbm, v_hbm, g_hbm, gate_ref, w_hbm,
    qg_ref, kg_ref, ig_ref, wg_ref,
    in_ref, q_ref, k_ref, v_ref, g_ref, w_ref,
    kv_in, qg_in, down_in, down_out, up_in, up_out, down_acc, up_acc,
    vg, vg_seq, x_all, w_all, part, part_in, sum_ref,
    gate_all, gate_pad, gate_t, gate_rev, soft, raised, value_dot,
    peaks, factors, row_terms, stats,
    local_sems, send_sems, recv_sems,
):
    s = lax.axis_index("sp")
    d = lax.axis_index("dp")
    core, x, y = d % 2, (d // 2) % 2, d // 4
    rows, model = in_ref.shape
    last = n - 1
    low, high = pl.ds(0, model // 2), pl.ds(model // 2, model // 2)
    block = model // n
    scale = HEAD_DIM ** (-0.5)
    f32, bf16 = jnp.float32, jnp.bfloat16

    fetched = [
        pltpu.make_async_copy(src, dst, local_sems.at[i])
        for i, (src, dst) in enumerate(
            ((k_hbm, k_ref), (q_hbm, q_ref), (in_hbm, in_ref), (w_hbm, w_ref), (v_hbm, v_ref), (g_hbm, g_ref))
        )
    ]
    for copy in fetched:
        copy.start()

    def near(step):
        return (
            d
            + (step % 2) * (1 - 2 * core)
            + ((step // 2) % 2) * (2 - 4 * x)
            + (step // 4) * (4 - 8 * y)
        )

    partner, x_near, y_near, corner = near(1), near(2), near(4), near(6)

    ids = {}
    used = [0]

    def sem(key, count=1):
        if key not in ids:
            ids[key] = used[0]
            used[0] += count
            assert used[0] <= recv_sems.shape[0], (key, used, recv_sems.shape)
        return ids[key]

    sent_ids = {}

    def remote(src, dst, kind, recv_id, to_sp, to_dp):
        send_id = sent_ids.setdefault(kind, len(sent_ids))
        assert send_id < send_sems.shape[0]
        return pltpu.make_async_remote_copy(
            src_ref=src,
            dst_ref=dst,
            send_sem=send_sems.at[send_id],
            recv_sem=recv_sems.at[recv_id],
            device_id={"sp": to_sp, "dp": to_dp},
            device_id_type=MESH,
        )

    def sent(kind, ref):
        remote(ref, ref, kind, 0, s, partner).wait_send()

    def arrived(name, ref):
        remote(ref, ref, "up", sem(name), s, partner).wait_recv()

    def up(si, a, b, p):
        src = (k_ref, v_ref)[a].at[:, lanes(p)] if b == si else kv_in.at[a, p, b]
        i = sem(("up", a, b), half) + p
        return remote(src, kv_in.at[a, p, b], "up", i, s + 1, d)

    def up_arrive(a, b, p):
        i = sem(("up", a, b), half) + p
        remote(kv_in.at[a, p, b], kv_in.at[a, p, b], "up", i, (s + 1) % n, d).wait_recv()

    def down(si, a, b, p):
        src = (q_ref, g_ref)[a].at[:, lanes(half + p)] if b == si else qg_in.at[a, p, last - b]
        i = sem(("down", a, b), half) + p
        return remote(src, qg_in.at[a, p, last - b], "down", i, s - 1, d)

    def down_arrive(a, b, p):
        i = sem(("down", a, b), half) + p
        remote(qg_in.at[a, p, last - b], qg_in.at[a, p, last - b], "down", i, (s + 1) % n, d).wait_recv()

    def down_sum(c, b, p):
        i = sem(("down sum", c, b), half) + p
        return remote(down_out.at[c, p, b], down_in.at[c, p, b], "down sum", i, (s + n - 1) % n, d)

    def up_sum(j, p):
        i = sem(("up sum", j), half) + p
        return remote(up_out.at[p, j], up_in.at[p, j], "up sum", i, (s + 1) % n, d)

    def gate_copy(sender, to):
        return remote(gate_ref, gate_all.at[sender], "gate", sem("gate"), to, d)

    def stat_width(a, b):
        return padded(rows * (n - max(a, b)))

    def stat_copy(which, sender, to):
        i = sem(("stat", which), n)
        piece = stats.at[which, sender, :, pl.ds(0, stat_width(sender, to))]
        return remote(piece, piece, ("stat", which), i + sender, to, d)

    def hop(si, b, upward):
        src = w_ref if b == si else w_all.at[d, b]
        i = sem(("hop", upward), n) + b
        return remote(src, w_all.at[d, b], ("hop", upward), i, (s + 1) % n if upward else (s + n - 1) % n, d)

    def vg_copy(p):
        return remote(vg.at[p], vg_seq.at[d], "vg", sem("vg"), s, p)

    def send_vg(p):
        @pl.when(d != p)
        def _():
            vg_copy(p).start()

        @pl.when(d == p)
        def _():
            vg_seq[p] = vg[p]

    def x_copy(name):
        src, dst, to = {
            "x low": (in_ref.at[:, low], x_all.at[d, :, low], x_near),
            "x high": (in_ref.at[:, high], x_all.at[d, :, high], x_near),
            "y high": (in_ref.at[:, high], x_all.at[d, :, high], y_near),
            "y low": (in_ref.at[:, low], x_all.at[d, :, low], y_near),
            "own": (in_ref, x_all.at[d], partner),
            "on y": (x_all.at[x_near, :, low],) * 2 + (y_near,),
            "on x": (x_all.at[y_near, :, high],) * 2 + (x_near,),
            "x over": (x_all.at[x_near],) * 2 + (partner,),
            "y over": (x_all.at[y_near],) * 2 + (partner,),
            "corner over": (x_all.at[corner],) * 2 + (partner,),
        }[name]
        key = "x on" if name[:2] == "on" else "x over" if name[-4:] == "over" or name == "own" else name
        return remote(src, dst, "x", sem(("x", key)), s, to)

    x_start = ("x low", "y high", "x high", "y low", "own")

    def x_middle():
        x_copy("x low").wait_recv()
        x_copy("on y").start()
        x_copy("y high").wait_recv()
        x_copy("on x").start()

    def x_over():
        x_copy("x high").wait_recv()
        x_copy("x over").start()
        x_copy("y low").wait_recv()
        x_copy("y over").start()

    def x_last():
        arrived(("x", "x on"), x_all.at[corner])
        x_copy("corner over").start()

    w_lower, w_upper = pl.ds(0, block // 2), pl.ds(block // 2, block // 2)

    def w_copy(name, j, own=False):
        first = w_ref if own else w_all.at[d, j]
        src, dst, to = {
            "x": (first, w_all.at[d, j], x_near),
            "y": (first, w_all.at[d, j], y_near),
            "own": (first, w_all.at[d, j], partner),
            "on y": (w_all.at[x_near, j, w_lower],) * 2 + (y_near,),
            "on x": (w_all.at[y_near, j, w_upper],) * 2 + (x_near,),
            "x over": (w_all.at[x_near, j],) * 2 + (partner,),
            "y over": (w_all.at[y_near, j],) * 2 + (partner,),
            "corner over": (w_all.at[corner, j],) * 2 + (partner,),
        }[name]
        if name[-4:] == "over" or name == "own":
            return remote(src, dst, "w", sem("w over", n) + j, s, to)
        key = ("on", j) if name[:2] == "on" else (name, j)
        return remote(src, dst, "w", sem(("w", key)), s, to)

    def w_start(j, own=False):
        for name in ("x", "y", "own"):
            w_copy(name, j, own).start()

    def w_middle(j):
        w_copy("x", j).wait_recv()
        w_copy("on y", j).start()
        w_copy("y", j).wait_recv()
        w_copy("on x", j).start()
        w_copy("x over", j).start()
        w_copy("y over", j).start()

    def w_last(j):
        arrived(("w", ("on", j)), w_all.at[corner, j])
        w_copy("corner over", j).start()

    def wide(buffer, a, p, count):
        return buffer[a, p, :count].astype(f32).reshape(count * rows, LANES)

    def own32(ref, p):
        return ref[:, lanes(p)].astype(f32)

    def gate_column(si, head):
        own = gate_t[rows * si : rows * si + rows]
        lane = lax.broadcasted_iota(jnp.int32, own.shape, 1)
        return jnp.sum(jnp.where(lane == head, own, 0.0), axis=1, keepdims=True)

    def softmax_queries(si, p):
        columns = rows * (si + 1)
        q32, g32 = own32(q_ref, p), own32(g_ref, p)
        keys = wide(kv_in, 0, p, si + 1).astype(bf16)
        total = None
        for h in range(2):
            head = 2 * p + h
            q_own, g_own = own_lanes(h, q32, g32)
            scores = dot(q_own, keys, BY_LANES) * scale
            scores = scores + gate_column(si, head) - gate_pad[pl.ds(head, 1), :columns]
            scores = causal(scores, rows, False)
            peak = jnp.max(scores, axis=1, keepdims=True)
            up_scores = jnp.exp(scores - peak)
            part_soft = up_scores * (1.0 / jnp.sum(up_scores, axis=1, keepdims=True))
            soft[head, :, :columns] = part_soft
            total = plus(total, dot(part_soft.astype(bf16), g_own, BY_ROWS))
        return total

    def gradient_queries(si, p):
        columns = rows * (si + 1)
        q32, g32 = own32(q_ref, p), own32(g_ref, p)
        keys32 = wide(kv_in, 0, p, si + 1)
        values = wide(kv_in, 1, p, si + 1).astype(bf16)
        dq = dk = None
        for h in range(2):
            q_own, g_own = own_lanes(h, q32, g32)
            (k_own,) = own_lanes(h, keys32)
            part_soft = soft[2 * p + h, :, :columns]
            soft_grad = dot(g_own, values, BY_LANES)
            row_term = jnp.sum(part_soft * soft_grad, axis=1, keepdims=True)
            score_low = (part_soft * (soft_grad - row_term)).astype(bf16)
            dq = plus(dq, dot(score_low, k_own, PLAIN))
            dk = plus(dk, dot(score_low, q_own, BY_ROWS))
        qg_ref[:, lanes(p)] = (dq * scale).astype(bf16)
        return dk * scale

    def softmax_keys(si, p):
        columns = rows * (n - si)
        k32 = own32(k_ref, half + p)
        queries = wide(qg_in, 0, p, n - si).astype(bf16)
        for h in range(2):
            row = 2 * p + h
            head = 2 * half + row
            (k_own,) = own_lanes(h, k32)
            scores = dot(k_own, queries, BY_LANES) * scale
            scores = scores + gate_rev[pl.ds(head, 1), :columns] - gate_column(si, head)
            scores = causal(scores, rows, True)
            peak = jnp.max(scores, axis=0, keepdims=True)
            up_scores = jnp.exp(scores - peak)
            raised[row, :, :columns] = up_scores
            peaks[pl.ds(row, 1), :columns] = peak
            stats[0, si, pl.ds(row, 1), :columns] = peak + jnp.log(
                jnp.sum(up_scores, axis=0, keepdims=True)
            )

    def stat_pieces(si, which, empty):
        width = padded(rows * (n - si))
        pieces = []
        for u in range(n):
            held = stat_width(si, u)
            piece = stats[which, u, :, :held]
            lane = lax.broadcasted_iota(jnp.int32, piece.shape, 1)
            piece = jnp.where(lane < rows * (n - u), piece, empty)
            if held < width:
                rest = jnp.full((piece.shape[0], width - held), empty, f32)
                piece = jnp.concatenate([piece, rest], axis=1)
            pieces.append(piece)
        return pieces, width

    def join_peaks(si):
        pieces, width = stat_pieces(si, 0, LOWEST)
        peak = functools.reduce(jnp.maximum, pieces)
        total = sum(jnp.exp(piece - peak) for piece in pieces)
        factors[:, :width] = jnp.exp(peaks[:, :width] - (peak + jnp.log(total)))

    def join_terms(si):
        pieces, width = stat_pieces(si, 1, 0.0)
        row_terms[:, :width] = sum(pieces)

    def value_keys(si, p):
        columns = rows * (n - si)
        g32 = wide(qg_in, 1, p, n - si)
        g_all = g32.astype(bf16)
        v32 = own32(v_ref, half + p)
        total = None
        for h in range(2):
            row = 2 * p + h
            (g_own,) = own_lanes(h, g32)
            (v_own,) = own_lanes(h, v32)
            part_soft = raised[row, :, :columns] * factors[pl.ds(row, 1), :columns]
            raised[row, :, :columns] = part_soft
            total = plus(total, dot(part_soft.astype(bf16), g_own, PLAIN))
            soft_grad = dot(v_own, g_all, BY_LANES)
            value_dot[row, :, :columns] = soft_grad
            stats[1, si, pl.ds(row, 1), :columns] = jnp.sum(part_soft * soft_grad, axis=0, keepdims=True)
        vg[half + p] = total.astype(bf16)
        send_vg(half + p)

    def gradient_keys(si, p):
        columns = rows * (n - si)
        q32 = wide(qg_in, 0, p, n - si)
        k32 = own32(k_ref, half + p)
        dq = dk = None
        for h in range(2):
            row = 2 * p + h
            (q_own,) = own_lanes(h, q32)
            (k_own,) = own_lanes(h, k32)
            term = row_terms[pl.ds(row, 1), :columns]
            score_low = (raised[row, :, :columns] * (value_dot[row, :, :columns] - term)).astype(bf16)
            dk = plus(dk, dot(score_low, q_own, PLAIN))
            dq = plus(dq, dot(score_low, k_own, BY_ROWS))
        kg_ref[:, lanes(half + p)] = (dk * scale).astype(bf16)
        return dq * scale

    def pass_down(si, c, p, total):
        for b in range(si + 1):
            value = total[rows * b : rows * (b + 1)]
            if si < last:
                down_sum(c, b, p).wait_recv()
                value = value + down_in[c, p, b].astype(f32)
            value = value.astype(bf16)
            if b < si:
                down_out[c, p, b] = value
                down_sum(c, b, p).start()
            elif c == 0:
                vg[p] = value
                send_vg(p)
            else:
                kg_ref[:, lanes(p)] = value

    def pass_up(si, p, total):
        for j in range(n - si):
            value = total[rows * j : rows * (j + 1)]
            if si > 0:
                up_sum(j, p).wait_recv()
                value = value + up_in[p, j].astype(f32)
            value = value.astype(bf16)
            if j < last - si:
                up_out[p, j] = value
                up_sum(j, p).start()
            else:
                qg_ref[:, lanes(half + p)] = value

    def each(body, begin=0, end=half):
        def step(p, carry):
            body(p)
            return carry

        lax.fori_loop(begin, end, step, 0)

    def relay_up(si, a, t, p):
        if si - t >= 0 and si < last:
            up_arrive(a, si - t, p)
            up(si, a, si - t, p).start()

    def relay_down(si, a, t, p):
        if si + t <= last and si > 0:
            down_arrive(a, si + t, p)
            down(si, a, si + t, p).start()

    def send_own(si, upward, begin, end):
        for p in range(begin, end):
            (up if upward else down)(si, 1, si, p).start()

    def relay(si, a, t):
        for p in range(half):
            relay_up(si, a, t, p)
            relay_down(si, a, t, p)

    def relay_first(si):
        if si in (0, last):
            return
        upper = 2 * si >= n
        relay(si, 0, 1)
        send_own(si, not upper, 0, half)
        for t in range(2, n):
            relay(si, 0, t)
        send_own(si, upper, 0, half)

    def w_relay_up(si, t):
        if si - t >= 0:
            hop(si, si - t, True).wait_recv()
            if si < last:
                hop(si, si - t, True).start()
            w_start(si - t)

    def w_relay_down(si, t):
        if si + t <= last:
            hop(si, si + t, False).wait_recv()
            if si > 0:
                hop(si, si + t, False).start()
            w_start(si + t)

    def w_relay(si, t):
        w_relay_up(si, t)
        w_relay_down(si, t)

    def w_blocks(si, t):
        return [b for b in (si - t, si + t) if 0 <= b <= last]

    def first(si):
        columns, query_columns = rows * (si + 1), rows * (n - si)
        others = [u for u in range(n) if u != si]
        for p in range(half):
            if si < last:
                up(si, 0, si, p).start()
            if si > 0:
                down(si, 0, si, p).start()
        for u in others:
            gate_copy(si, u).start()
        if si == 0:
            send_own(si, True, 0, half)
            hop(si, si, True).start()
        if si == last:
            send_own(si, False, 0, half)
            hop(si, si, False).start()
        for name in x_start:
            x_copy(name).start()
        w_start(si, True)

        for p in range(half):
            for a, ref in enumerate((k_ref, v_ref)):
                kv_in[a, p, si] = ref[:, lanes(p)]
            for a, ref in enumerate((q_ref, g_ref)):
                qg_in[a, p, last - si] = ref[:, lanes(half + p)]
        relay_first(si)

        gate_pad[...] = jnp.zeros_like(gate_pad)
        for which in range(2):
            stats[which, si] = jnp.zeros(stats.shape[2:], f32)
        peaks[...] = jnp.zeros_like(peaks)
        held = gate_ref.shape[0]
        length = rows * n
        gate_pad[held * si : held * si + held, :length] = gate_ref[...]
        arrived("gate", gate_all.at[:last])
        for u in others:
            gate_pad[held * u : held * u + held, :length] = gate_all[u]
        turned = gate_pad[...].T
        gate_t[...] = turned
        back = [turned[rows * b : rows * (b + 1)] for b in reversed(range(n))]
        gate_rev[...] = jnp.concatenate(back + [turned[length:]], axis=0).T

        def queries_step(p):
            relay_up(si, 1, 1, p)
            if si == last:
                for b in range(si):
                    up_arrive(0, b, p)
            total = softmax_queries(si, p)
            if si == last:
                pass_down(si, 0, p, total)
            else:
                down_acc[0, p, : si + 1] = total.reshape(si + 1, rows, LANES)

        def keys_step(p):
            if 2 * si >= n:
                relay_down(si, 1, 1, p)
            if si == 0:
                for b in range(1, n):
                    down_arrive(0, b, p)
            softmax_keys(si, p)

        def gradient_step(p):
            if si == last:
                for b in range(si):
                    up_arrive(1, b, p)
            total = gradient_queries(si, p)
            if si == last:
                pass_down(si, 1, p, total)
            else:
                down_acc[1, p, : si + 1] = total.reshape(si + 1, rows, LANES)

        def do_keys():
            each(keys_step)
            for u in others:
                stat_copy(0, si, u).start()

        if si == 0:
            each(queries_step)
            do_keys()
            each(gradient_step)
        elif 2 * si < n:
            each(queries_step)
            do_keys()
            for p in range(half):
                relay_down(si, 1, 1, p)
            hop(si, si, True).start()
        elif si < last:
            do_keys()
            hop(si, si, False).start()
            each(queries_step)
        else:
            do_keys()
            each(queries_step)
        x_middle()
        for t in range(2, n):
            relay(si, 1, t)
        if 0 < si < last:
            if 2 * si < n:
                hop(si, si, False).start()
                w_relay_up(si, 1)
            else:
                hop(si, si, True).start()
        x_all[d] = in_ref[...]
        w_all[d, si] = w_ref[...]

        def value_step(p):
            if si == 0:
                for b in range(1, n):
                    down_arrive(1, b, p)
            value_keys(si, p)

        def do_values():
            for u in others:
                stat_copy(0, u, si).wait_recv()
            join_peaks(si)
            each(value_step)
            for u in others:
                stat_copy(1, si, u).start()

        def value_sums(begin=0, end=half):
            each(lambda p: pass_down(si, 0, p, down_acc[0, p, : si + 1].reshape(columns, LANES)), begin, end)

        def key_gradient_step(p):
            total = gradient_keys(si, p)
            if si == 0:
                pass_up(si, p, total)
            else:
                up_acc[p, : n - si] = total.reshape(n - si, rows, LANES)

        def do_key_gradients():
            for u in others:
                stat_copy(1, u, si).wait_recv()
            join_terms(si)
            each(key_gradient_step)

        if si == 0:
            do_values()
            x_over()
            w_middle(si)
            w_relay(si, 1)
            do_key_gradients()
            value_sums()
            x_last()
            w_relay(si, 2)
        elif si == last:
            do_values()
            x_over()
            w_middle(si)
            each(gradient_step)
            x_last()
            w_relay(si, 1)
            do_key_gradients()
            w_relay(si, 2)
        elif 2 * si < n:
            do_values()
            x_over()
            w_middle(si)
            each(gradient_step)
            value_sums()
            w_relay_down(si, 1)
            x_last()
            do_key_gradients()
            w_relay(si, 2)
            chain_first(si, 0, half // 2)
        else:
            value_sums(0, half // 2)
            do_values()
            value_sums(half // 2, half - 1)
            each(gradient_step, 0, half // 2)
            value_sums(half - 1, half)
            w_relay_down(si, 1)
            x_over()
            w_middle(si)
            w_relay_up(si, 1)
            each(gradient_step, half // 2, half)
            x_last()
            do_key_gradients()
            chain_first(si, 0, half // 2)
            w_relay(si, 2)

    def chain_down(si, begin, end):
        if si < last:
            for p in range(begin, end):
                pass_down(si, 1, p, down_acc[1, p, : si + 1].reshape(rows * (si + 1), LANES))

    def chain_up(si, begin, end):
        if si > 0:
            for p in range(begin, end):
                pass_up(si, p, up_acc[p, : n - si].reshape(rows * (n - si), LANES))

    def chain_first(si, begin, end):
        (chain_up if 2 * si < n else chain_down)(si, begin, end)

    def chain_rest(si):
        if si == 0:
            chain_down(si, 0, half)
        elif 2 * si >= n:
            chain_up(si, 0, half)

    def fourth(si):
        w_relay(si, 3)
        w_last(si)

    def fifth(si):
        for j in w_blocks(si, 1):
            w_middle(j)

    def sixth(si):
        for j in w_blocks(si, 2):
            w_middle(j)
        for j in w_blocks(si, 1):
            w_last(j)
        for j in w_blocks(si, 3):
            w_middle(j)

    def seventh(si):
        chain_rest(si)
        for t in (2, 3):
            for j in w_blocks(si, t):
                w_last(j)

    def finish(si):
        if si < last:
            sent("up", kv_in.at[:, :, : si + 1])
            sent("up sum", up_out.at[:, : last - si])
            sent(("hop", True), w_all.at[0, : si + 1])
        if si > 0:
            sent("down", qg_in.at[:, :, : n - si])
            sent("down sum", down_out.at[:, :, :si])
            sent(("hop", False), w_all.at[0, : n - si])
        width = sum(stat_width(si, u) for u in range(n) if u != si)
        count = next(c for c in range(1, n + 1) if width % (c * LANES) == 0 and width // c <= stats.shape[3])
        for which in range(2):
            sent(("stat", which), stats.at[0, :count, :, : width // count])

    def by_device(body):
        for si in range(n):
            @pl.when(s == si)
            def _():
                body(si)

    barrier = pltpu.get_barrier_semaphore()
    for r in range(1, n):
        pl.semaphore_signal(barrier, inc=1, device_id={"sp": (s + r) % n, "dp": d}, device_id_type=MESH)
    for step in range(1, 8):
        pl.semaphore_signal(barrier, inc=1, device_id={"sp": s, "dp": near(step)}, device_id_type=MESH)
    pl.semaphore_wait(barrier, n - 1 + 7)
    for copy in fetched:
        copy.wait()

    by_device(first)

    arrived(("x", "x over"), x_all.at[:4])
    arrived("vg", vg_seq.at[:7])

    def weight_part(j):
        columns = pl.ds(pl.multiple_of(j * block, LANES), block)
        total = None
        for i in range(8):
            total = plus(total, dot(vg_seq[i], x_all[i, :, columns], BY_ROWS))
        return total

    side = s // 2
    mate = s + 1 - 2 * (s % 2)
    outer = (s == 0) | (s == last)
    inner = (s > 0) & (s < last)
    outermost, nearest = (1 - side) * last, 2 - side

    def part_copy(j, slot, to):
        return remote(part.at[j], part_in.at[slot], "part", sem("part", 4) + slot, to, d)

    def give(j, k, slot):
        part[j] = sum_ref[k].astype(bf16)
        part_copy(j, slot, mate).start()

    sum_ref[0] = weight_part(jnp.where(outer, outermost, mate))
    pl.when(outer)(lambda: give(outermost, 0, 0))
    pl.when(inner)(lambda: give(mate, 0, 2))
    sum_ref[1] = weight_part(jnp.where(outer, nearest, outermost))
    pl.when(outer)(lambda: give(nearest, 1, 1))
    by_device(fourth)
    sum_ref[2] = weight_part(jnp.where(outer, mate, nearest))
    pl.when(outer)(lambda: give(mate, 2, 2))
    sum_ref[3] = weight_part(s)
    by_device(lambda si: chain_first(si, half // 2, half))
    by_device(fifth)

    def pass_part(k, j):
        part_copy(j, k, j).wait_recv()
        part[j] = (sum_ref[k + 1] + part_in[k].astype(f32)).astype(bf16)
        part_copy(j, 3, j).start()

    def input_part(j):
        remote(w_all.at[:4, j], w_all.at[:4, j], "w", sem("w over", n) + j, s, partner).wait_recv()
        vg_rows = jnp.concatenate([vg[i] for i in range(8)], axis=1)
        w_rows = jnp.concatenate([w_all[i, j] for i in range(8)], axis=1)
        columns = pl.ds(pl.multiple_of(j * block, LANES), block)
        ig_ref[:, columns] = dot(vg_rows, w_rows, BY_LANES).astype(bf16)

    input_part(s)
    for step, j in enumerate((outermost, nearest)):
        by_device(lambda si: 0 < 2 * si < n and chain_down(si, step * half // 2, (step + 1) * half // 2))
        pl.when(inner)(lambda: pass_part(step, j))

    by_device(sixth)
    input_part(mate)
    by_device(seventh)
    input_part(nearest)
    input_part(outermost)

    by_device(finish)
    sent("gate", gate_all.at[:last])
    sent("vg", vg_seq.at[:7])
    sent("x", x_all.at[:7])
    sent("w", w_all.at[:7])

    for slot in (2, 3):
        part_copy(s, slot, mate).wait_recv()
    total = sum_ref[3] + part_in[2].astype(f32) + part_in[3].astype(f32)
    wg_ref[...] = total.T
    sent("part", part.at[:3])


def put_out(*refs):
    sems = refs[-1]
    copies = [pltpu.make_async_copy(refs[i], refs[4 + i], sems.at[i]) for i in range(4)]
    for copy in copies:
        copy.start()
    for copy in copies:
        copy.wait()


def fused(mesh, inputs, query, key, value, cotangent, gate, weight):
    n = mesh.shape["sp"]
    rows, width = query.shape[1:]
    model = inputs.shape[2]
    half = width // LANES // 2
    length = n * rows
    wide = padded(length)
    bf16, f32 = jnp.bfloat16, jnp.float32
    copies = 7 * (n - 1) * half + 8 * n + 12
    vmem = pl.BlockSpec(memory_space=pltpu.VMEM)
    hbm = pl.BlockSpec(memory_space=pl.ANY)
    results = (
        jax.ShapeDtypeStruct((rows, width), bf16),
        jax.ShapeDtypeStruct((rows, width), bf16),
        jax.ShapeDtypeStruct((rows, model), bf16),
        jax.ShapeDtypeStruct((model // n, LANES), f32),
    )
    outs = pl.pallas_call(
        functools.partial(kernel, n, half),
        out_shape=tuple(pltpu.VMEM(x.shape, x.dtype) for x in results),
        in_specs=[hbm] * 5 + [vmem, hbm],
        out_specs=(vmem,) * 4,
        scratch_shapes=[
            pltpu.VMEM((rows, model), bf16),
            *[pltpu.VMEM((rows, width), bf16)] * 4,
            pltpu.VMEM((model // n, LANES), bf16),
            *[pltpu.VMEM((2, half, n, rows, LANES), bf16)] * 2,
            *[pltpu.VMEM((2, half, n - 1, rows, LANES), bf16)] * 2,
            *[pltpu.VMEM((half, n - 1, rows, LANES), bf16)] * 2,
            pltpu.VMEM((2, half, n, rows, LANES), f32),
            pltpu.VMEM((half, n, rows, LANES), f32),
            pltpu.VMEM((8, rows, LANES), bf16),
            pltpu.VMEM((8, rows, LANES), bf16),
            pltpu.VMEM((8, rows, model), bf16),
            pltpu.VMEM((8, n, model // n, LANES), bf16),
            pltpu.VMEM((n, LANES, model // n), bf16),
            pltpu.VMEM((4, LANES, model // n), bf16),
            pltpu.VMEM((4, LANES, model // n), f32),
            pltpu.VMEM((n, gate.shape[1], length), f32),
            pltpu.VMEM((LANES, wide), f32),
            pltpu.VMEM((wide, LANES), f32),
            pltpu.VMEM((LANES, wide), f32),
            *[pltpu.VMEM((2 * half, rows, length), f32)] * 3,
            *[pltpu.VMEM((2 * half, wide), f32)] * 3,
            pltpu.VMEM((2, n, 2 * half, wide), f32),
            pltpu.SemaphoreType.DMA((6,)),
            pltpu.SemaphoreType.DMA((13,)),
            pltpu.SemaphoreType.DMA((copies,)),
        ],
        compiler_params=pltpu.CompilerParams(
            collective_id=0, has_side_effects=True, vmem_limit_bytes=60 * 2**20
        ),
    )(inputs[0], query[0], key[0], value[0], cotangent[0], gate[0], weight)
    query_grad, key_grad, input_grad, weight_grad = pl.pallas_call(
        put_out,
        out_shape=results,
        in_specs=[vmem] * 4,
        out_specs=(hbm,) * 4,
        scratch_shapes=[pltpu.SemaphoreType.DMA((4,))],
        compiler_params=pltpu.CompilerParams(vmem_limit_bytes=2**20),
    )(*(pltpu.with_memory_space_constraint(x, pltpu.VMEM) for x in outs))
    return (query_grad[None], key_grad[None], input_grad[None], weight_grad)


def solution(mesh):
    in_specs = (
        P("dp", "sp", None),
        P("dp", "sp", None),
        P("dp", "sp", None),
        P("dp", "sp", None),
        P("dp", "sp", None),
        P("dp", "sp", None),
        P("sp", "dp"),
    )
    out_specs = (P("dp", "sp", None), P("dp", "sp", None), P("dp", "sp", None), P("sp", "dp"))
    sp_count, dp_count = mesh.shape["sp"], mesh.shape["dp"]

    def per_device(*arrays):
        if one_kernel_fits(sp_count, dp_count, *arrays):
            return fused(mesh, *arrays)
        return shards(*arrays)

    return jax.shard_map(per_device, mesh=mesh, in_specs=in_specs, out_specs=out_specs, check_vma=False)
```

```python
import functools

import jax
import jax.numpy as jnp
from jax import lax
from jax.experimental import pallas as pl
from jax.experimental.pallas import tpu as pltpu
from jax.sharding import PartitionSpec as P

HEAD_DIM = 64


def attention_backward(query_heads, key_heads, value_heads, grad_heads, prefix):
    length = query_heads.shape[0]
    score_scale = HEAD_DIM ** (-0.5)
    block_count = max(1, length // 512)
    block_rows = length // block_count
    key_accum = jnp.zeros(key_heads.shape, jnp.float32)
    value_accum = jnp.zeros(key_heads.shape, jnp.float32)
    query_parts = []
    for block_index in range(block_count):
        first_row = block_index * block_rows
        last_row = first_row + block_rows
        query_rows = query_heads[first_row:last_row]
        key_rows = key_heads[:last_row]
        grad_rows = grad_heads[first_row:last_row]
        scores = (
            jnp.einsum("qhd,khd->hqk", query_rows, key_rows, preferred_element_type=jnp.float32)
            * score_scale
        )
        scores = scores + prefix[:, first_row:last_row, None] - prefix[:, None, :last_row]
        causal = jnp.arange(last_row)[None, :] <= (first_row + jnp.arange(block_rows))[:, None]
        scores = jnp.where(causal[None], scores, -jnp.inf)
        row_peak = jnp.max(scores, axis=-1, keepdims=True)
        raised_scores = jnp.exp(scores - row_peak)
        softmax_rows = raised_scores / jnp.sum(raised_scores, axis=-1, keepdims=True)
        softmax_low = softmax_rows.astype(jnp.bfloat16)
        value_accum = value_accum.at[:last_row].add(
            jnp.einsum("hqk,qhd->khd", softmax_low, grad_rows, preferred_element_type=jnp.float32)
        )
        softmax_grad = jnp.einsum(
            "qhd,khd->hqk", grad_rows, value_heads[:last_row], preferred_element_type=jnp.float32
        )
        row_term = jnp.sum(softmax_rows * softmax_grad, axis=-1, keepdims=True)
        score_low = (softmax_rows * (softmax_grad - row_term)).astype(jnp.bfloat16)
        query_parts.append(
            (
                jnp.einsum("hqk,khd->qhd", score_low, key_rows, preferred_element_type=jnp.float32)
                * score_scale
            ).astype(jnp.bfloat16)
        )
        key_accum = key_accum.at[:last_row].add(
            jnp.einsum("hqk,qhd->khd", score_low, query_rows, preferred_element_type=jnp.float32)
        )
    query_grad = jnp.concatenate(query_parts, axis=0)
    key_grad = (key_accum * score_scale).astype(jnp.bfloat16)
    return (query_grad, key_grad, value_accum.astype(jnp.bfloat16))


def shards(inputs, query_vectors, key_vectors, value_vectors, cotangent, gate_prefix, value_weight):
    query_seq, key_seq, value_seq, grad_seq, input_cols = (
        lax.all_to_all(query_vectors[0], "sp", split_axis=1, concat_axis=0, tiled=True),
        lax.all_to_all(key_vectors[0], "sp", split_axis=1, concat_axis=0, tiled=True),
        lax.all_to_all(value_vectors[0], "sp", split_axis=1, concat_axis=0, tiled=True),
        lax.all_to_all(cotangent[0], "sp", split_axis=1, concat_axis=0, tiled=True),
        lax.all_to_all(inputs[0], "sp", split_axis=1, concat_axis=0, tiled=True),
    )
    length = query_seq.shape[0]
    local_width = query_seq.shape[1]
    head_shape = (length, local_width // HEAD_DIM, HEAD_DIM)
    query_heads, key_heads, value_heads = attention_backward(
        query_seq.reshape(head_shape),
        key_seq.reshape(head_shape),
        value_seq.reshape(head_shape),
        grad_seq.reshape(head_shape),
        gate_prefix[0],
    )
    query_flat = query_heads.reshape(length, local_width)
    key_flat = key_heads.reshape(length, local_width)
    value_flat = value_heads.reshape(length, local_width)
    value_all = lax.all_gather(value_flat, "sp", axis=1, tiled=True)
    weight_block = lax.all_gather(value_weight, "dp", axis=1, tiled=True)
    weight_rows = lax.psum_scatter(
        lax.dot_general(
            value_all, input_cols, (((0,), (0,)), ((), ())), preferred_element_type=jnp.float32
        ).astype(jnp.bfloat16),
        "dp",
        scatter_dimension=0,
        tiled=True,
    ).astype(jnp.float32)
    weight_grad = weight_rows.T
    query_back, key_back = (
        lax.all_to_all(query_flat, "sp", split_axis=0, concat_axis=1, tiled=True),
        lax.all_to_all(key_flat, "sp", split_axis=0, concat_axis=1, tiled=True),
    )
    column_grad = lax.dot_general(
        value_all, weight_block, (((1,), (1,)), ((), ())), preferred_element_type=jnp.float32
    ).astype(jnp.bfloat16)
    input_grad = lax.all_to_all(column_grad, "sp", split_axis=0, concat_axis=1, tiled=True)
    return (query_back[None], key_back[None], input_grad[None], weight_grad)


LANES = 128
MESH = pl.DeviceIdType.MESH


def one_kernel_fits(sp_count, dp_count, inputs, query, key, value, cotangent, gate, weight):
    rows, width = query.shape[1:]
    model = inputs.shape[2]
    return (
        dp_count == 8
        and width == dp_count * LANES
        and width % (sp_count * LANES) == 0
        and gate.shape[1] * sp_count * HEAD_DIM == width
        and gate.shape[2] == rows * sp_count
        and LANES == 2 * HEAD_DIM
        and rows % 8 == 0
        and model % (sp_count * LANES) == 0
        and model % (2 * LANES) == 0
        and sp_count == 4
        and rows * sp_count <= 1024
        and (dp_count * rows + width) * model <= 3 * 2**21
    )


dot = functools.partial(lax.dot_general, preferred_element_type=jnp.float32)
BY_LANES = (((1,), (1,)), ((), ()))
BY_ROWS = (((0,), (0,)), ((), ()))
PLAIN = (((1,), (0,)), ((), ()))
LOWEST = -1e30


def own_lanes(head, *arrays):
    lane = lax.broadcasted_iota(jnp.int32, arrays[0].shape, 1)
    own = (lane < HEAD_DIM) if head == 0 else (lane >= HEAD_DIM)
    return [jnp.where(own, x, 0.0).astype(jnp.bfloat16) for x in arrays]


def lanes(p):
    return pl.ds(p * LANES if isinstance(p, int) else pl.multiple_of(p * LANES, LANES), LANES)


def padded(columns):
    return -(-columns // LANES) * LANES


def plus(total, term):
    return term if total is None else total + term


def causal(scores, rows, keys_first):
    columns = scores.shape[1]
    start = columns - rows
    low = start // LANES * LANES
    tail = scores[:, low:]
    row = lax.broadcasted_iota(jnp.int32, tail.shape, 0)
    column = lax.broadcasted_iota(jnp.int32, tail.shape, 1) + (low - start)
    kept = ((column >= row) | (column < 0)) if keys_first else (column <= row)
    tail = jnp.where(kept, tail, -jnp.inf)
    return jnp.concatenate([scores[:, :low], tail], axis=1) if low else tail


def kernel(
    n, half, in_hbm, q_hbm, k_hbm, v_hbm, g_hbm, gate_ref, w_hbm,
    qg_ref, kg_ref, ig_ref, wg_ref,
    in_ref, q_ref, k_ref, v_ref, g_ref, w_ref,
    kv_in, qg_in, down_in, down_out, up_in, up_out, down_acc, up_acc,
    vg, vg_seq, x_all, w_all, part, part_in, sum_ref,
    gate_all, gate_pad, gate_t, gate_rev, soft, raised, value_dot,
    peaks, factors, row_terms, stats,
    local_sems, send_sems, recv_sems,
):
    s = lax.axis_index("sp")
    d = lax.axis_index("dp")
    core, x, y = d % 2, (d // 2) % 2, d // 4
    rows, model = in_ref.shape
    last = n - 1
    low, high = pl.ds(0, model // 2), pl.ds(model // 2, model // 2)
    block = model // n
    scale = HEAD_DIM ** (-0.5)
    f32, bf16 = jnp.float32, jnp.bfloat16

    fetched = [
        pltpu.make_async_copy(src, dst, local_sems.at[i])
        for i, (src, dst) in enumerate(
            ((k_hbm, k_ref), (q_hbm, q_ref), (in_hbm, in_ref), (w_hbm, w_ref), (v_hbm, v_ref), (g_hbm, g_ref))
        )
    ]
    for copy in fetched:
        copy.start()

    def near(step):
        return (
            d
            + (step % 2) * (1 - 2 * core)
            + ((step // 2) % 2) * (2 - 4 * x)
            + (step // 4) * (4 - 8 * y)
        )

    partner, x_near, y_near, corner = near(1), near(2), near(4), near(6)

    ids = {}
    used = [0]

    def sem(key, count=1):
        if key not in ids:
            ids[key] = used[0]
            used[0] += count
            assert used[0] <= recv_sems.shape[0], (key, used, recv_sems.shape)
        return ids[key]

    sent_ids = {}

    def remote(src, dst, kind, recv_id, to_sp, to_dp):
        send_id = sent_ids.setdefault(kind, len(sent_ids))
        assert send_id < send_sems.shape[0]
        return pltpu.make_async_remote_copy(
            src_ref=src,
            dst_ref=dst,
            send_sem=send_sems.at[send_id],
            recv_sem=recv_sems.at[recv_id],
            device_id={"sp": to_sp, "dp": to_dp},
            device_id_type=MESH,
        )

    def sent(kind, ref):
        remote(ref, ref, kind, 0, s, partner).wait_send()

    def arrived(name, ref):
        remote(ref, ref, "up", sem(name), s, partner).wait_recv()

    def up(si, a, b, p):
        src = (k_ref, v_ref)[a].at[:, lanes(p)] if b == si else kv_in.at[a, p, b]
        i = sem(("up", a, b), half) + p
        return remote(src, kv_in.at[a, p, b], "up", i, s + 1, d)

    def up_arrive(a, b, p):
        i = sem(("up", a, b), half) + p
        remote(kv_in.at[a, p, b], kv_in.at[a, p, b], "up", i, (s + 1) % n, d).wait_recv()

    def down(si, a, b, p):
        src = (q_ref, g_ref)[a].at[:, lanes(half + p)] if b == si else qg_in.at[a, p, last - b]
        i = sem(("down", a, b), half) + p
        return remote(src, qg_in.at[a, p, last - b], "down", i, s - 1, d)

    def down_arrive(a, b, p):
        i = sem(("down", a, b), half) + p
        remote(qg_in.at[a, p, last - b], qg_in.at[a, p, last - b], "down", i, (s + 1) % n, d).wait_recv()

    def down_sum(c, b, p):
        i = sem(("down sum", c, b), half) + p
        return remote(down_out.at[c, p, b], down_in.at[c, p, b], "down sum", i, (s + n - 1) % n, d)

    def up_sum(j, p):
        i = sem(("up sum", j), half) + p
        return remote(up_out.at[p, j], up_in.at[p, j], "up sum", i, (s + 1) % n, d)

    def gate_copy(sender, to):
        return remote(gate_ref, gate_all.at[sender], "gate", sem("gate"), to, d)

    def stat_width(a, b):
        return padded(rows * (n - max(a, b)))

    def stat_copy(which, sender, to):
        i = sem(("stat", which), n)
        piece = stats.at[which, sender, :, pl.ds(0, stat_width(sender, to))]
        return remote(piece, piece, ("stat", which), i + sender, to, d)

    def hop(si, b, upward):
        src = w_ref if b == si else w_all.at[d, b]
        i = sem(("hop", upward), n) + b
        return remote(src, w_all.at[d, b], ("hop", upward), i, (s + 1) % n if upward else (s + n - 1) % n, d)

    def vg_copy(p):
        return remote(vg.at[p], vg_seq.at[d], "vg", sem("vg"), s, p)

    def send_vg(p):
        @pl.when(d != p)
        def _():
            vg_copy(p).start()

        @pl.when(d == p)
        def _():
            vg_seq[p] = vg[p]

    def x_copy(name):
        src, dst, to = {
            "x low": (in_ref.at[:, low], x_all.at[d, :, low], x_near),
            "x high": (in_ref.at[:, high], x_all.at[d, :, high], x_near),
            "y high": (in_ref.at[:, high], x_all.at[d, :, high], y_near),
            "y low": (in_ref.at[:, low], x_all.at[d, :, low], y_near),
            "own": (in_ref, x_all.at[d], partner),
            "on y": (x_all.at[x_near, :, low],) * 2 + (y_near,),
            "on x": (x_all.at[y_near, :, high],) * 2 + (x_near,),
            "x over": (x_all.at[x_near],) * 2 + (partner,),
            "y over": (x_all.at[y_near],) * 2 + (partner,),
            "corner over": (x_all.at[corner],) * 2 + (partner,),
        }[name]
        key = "x on" if name[:2] == "on" else "x over" if name[-4:] == "over" or name == "own" else name
        return remote(src, dst, "x", sem(("x", key)), s, to)

    x_start = ("x low", "y high", "x high", "y low", "own")

    def x_middle():
        x_copy("x low").wait_recv()
        x_copy("on y").start()
        x_copy("y high").wait_recv()
        x_copy("on x").start()

    def x_over():
        x_copy("x high").wait_recv()
        x_copy("x over").start()
        x_copy("y low").wait_recv()
        x_copy("y over").start()

    def x_last():
        arrived(("x", "x on"), x_all.at[corner])
        x_copy("corner over").start()

    w_lower, w_upper = pl.ds(0, block // 2), pl.ds(block // 2, block // 2)

    def w_copy(name, j, own=False):
        first = w_ref if own else w_all.at[d, j]
        src, dst, to = {
            "x": (first, w_all.at[d, j], x_near),
            "y": (first, w_all.at[d, j], y_near),
            "own": (first, w_all.at[d, j], partner),
            "on y": (w_all.at[x_near, j, w_lower],) * 2 + (y_near,),
            "on x": (w_all.at[y_near, j, w_upper],) * 2 + (x_near,),
            "x over": (w_all.at[x_near, j],) * 2 + (partner,),
            "y over": (w_all.at[y_near, j],) * 2 + (partner,),
            "corner over": (w_all.at[corner, j],) * 2 + (partner,),
        }[name]
        if name[-4:] == "over" or name == "own":
            return remote(src, dst, "w", sem("w over", n) + j, s, to)
        key = ("on", j) if name[:2] == "on" else (name, j)
        return remote(src, dst, "w", sem(("w", key)), s, to)

    def w_start(j, own=False):
        for name in ("x", "y", "own"):
            w_copy(name, j, own).start()

    def w_middle(j):
        w_copy("x", j).wait_recv()
        w_copy("on y", j).start()
        w_copy("y", j).wait_recv()
        w_copy("on x", j).start()
        w_copy("x over", j).start()
        w_copy("y over", j).start()

    def w_last(j):
        arrived(("w", ("on", j)), w_all.at[corner, j])
        w_copy("corner over", j).start()

    def wide(buffer, a, p, count):
        return buffer[a, p, :count].astype(f32).reshape(count * rows, LANES)

    def own32(ref, p):
        return ref[:, lanes(p)].astype(f32)

    def gate_column(si, head):
        own = gate_t[rows * si : rows * si + rows]
        lane = lax.broadcasted_iota(jnp.int32, own.shape, 1)
        return jnp.sum(jnp.where(lane == head, own, 0.0), axis=1, keepdims=True)

    def softmax_queries(si, p):
        columns = rows * (si + 1)
        q32, g32 = own32(q_ref, p), own32(g_ref, p)
        keys = wide(kv_in, 0, p, si + 1).astype(bf16)
        total = None
        for h in range(2):
            head = 2 * p + h
            q_own, g_own = own_lanes(h, q32, g32)
            scores = dot(q_own, keys, BY_LANES) * scale
            scores = scores + gate_column(si, head) - gate_pad[pl.ds(head, 1), :columns]
            scores = causal(scores, rows, False)
            peak = jnp.max(scores, axis=1, keepdims=True)
            up_scores = jnp.exp(scores - peak)
            part_soft = up_scores * (1.0 / jnp.sum(up_scores, axis=1, keepdims=True))
            soft[head, :, :columns] = part_soft
            total = plus(total, dot(part_soft.astype(bf16), g_own, BY_ROWS))
        return total

    def gradient_queries(si, p):
        columns = rows * (si + 1)
        q32, g32 = own32(q_ref, p), own32(g_ref, p)
        keys32 = wide(kv_in, 0, p, si + 1)
        values = wide(kv_in, 1, p, si + 1).astype(bf16)
        dq = dk = None
        for h in range(2):
            q_own, g_own = own_lanes(h, q32, g32)
            (k_own,) = own_lanes(h, keys32)
            part_soft = soft[2 * p + h, :, :columns]
            soft_grad = dot(g_own, values, BY_LANES)
            row_term = jnp.sum(part_soft * soft_grad, axis=1, keepdims=True)
            score_low = (part_soft * (soft_grad - row_term)).astype(bf16)
            dq = plus(dq, dot(score_low, k_own, PLAIN))
            dk = plus(dk, dot(score_low, q_own, BY_ROWS))
        qg_ref[:, lanes(p)] = (dq * scale).astype(bf16)
        return dk * scale

    def softmax_keys(si, p):
        columns = rows * (n - si)
        k32 = own32(k_ref, half + p)
        queries = wide(qg_in, 0, p, n - si).astype(bf16)
        for h in range(2):
            row = 2 * p + h
            head = 2 * half + row
            (k_own,) = own_lanes(h, k32)
            scores = dot(k_own, queries, BY_LANES) * scale
            scores = scores + gate_rev[pl.ds(head, 1), :columns] - gate_column(si, head)
            scores = causal(scores, rows, True)
            peak = jnp.max(scores, axis=0, keepdims=True)
            up_scores = jnp.exp(scores - peak)
            raised[row, :, :columns] = up_scores
            peaks[pl.ds(row, 1), :columns] = peak
            stats[0, si, pl.ds(row, 1), :columns] = peak + jnp.log(
                jnp.sum(up_scores, axis=0, keepdims=True)
            )

    def stat_pieces(si, which, empty):
        width = padded(rows * (n - si))
        pieces = []
        for u in range(n):
            held = stat_width(si, u)
            piece = stats[which, u, :, :held]
            lane = lax.broadcasted_iota(jnp.int32, piece.shape, 1)
            piece = jnp.where(lane < rows * (n - u), piece, empty)
            if held < width:
                rest = jnp.full((piece.shape[0], width - held), empty, f32)
                piece = jnp.concatenate([piece, rest], axis=1)
            pieces.append(piece)
        return pieces, width

    def join_peaks(si):
        pieces, width = stat_pieces(si, 0, LOWEST)
        peak = functools.reduce(jnp.maximum, pieces)
        total = sum(jnp.exp(piece - peak) for piece in pieces)
        factors[:, :width] = jnp.exp(peaks[:, :width] - (peak + jnp.log(total)))

    def join_terms(si):
        pieces, width = stat_pieces(si, 1, 0.0)
        row_terms[:, :width] = sum(pieces)

    def value_keys(si, p):
        columns = rows * (n - si)
        g32 = wide(qg_in, 1, p, n - si)
        g_all = g32.astype(bf16)
        v32 = own32(v_ref, half + p)
        total = None
        for h in range(2):
            row = 2 * p + h
            (g_own,) = own_lanes(h, g32)
            (v_own,) = own_lanes(h, v32)
            part_soft = raised[row, :, :columns] * factors[pl.ds(row, 1), :columns]
            raised[row, :, :columns] = part_soft
            total = plus(total, dot(part_soft.astype(bf16), g_own, PLAIN))
            soft_grad = dot(v_own, g_all, BY_LANES)
            value_dot[row, :, :columns] = soft_grad
            stats[1, si, pl.ds(row, 1), :columns] = jnp.sum(part_soft * soft_grad, axis=0, keepdims=True)
        vg[half + p] = total.astype(bf16)
        send_vg(half + p)

    def gradient_keys(si, p):
        columns = rows * (n - si)
        q32 = wide(qg_in, 0, p, n - si)
        k32 = own32(k_ref, half + p)
        dq = dk = None
        for h in range(2):
            row = 2 * p + h
            (q_own,) = own_lanes(h, q32)
            (k_own,) = own_lanes(h, k32)
            term = row_terms[pl.ds(row, 1), :columns]
            score_low = (raised[row, :, :columns] * (value_dot[row, :, :columns] - term)).astype(bf16)
            dk = plus(dk, dot(score_low, q_own, PLAIN))
            dq = plus(dq, dot(score_low, k_own, BY_ROWS))
        kg_ref[:, lanes(half + p)] = (dk * scale).astype(bf16)
        return dq * scale

    def pass_down(si, c, p, total):
        for b in range(si + 1):
            value = total[rows * b : rows * (b + 1)]
            if si < last:
                down_sum(c, b, p).wait_recv()
                value = value + down_in[c, p, b].astype(f32)
            value = value.astype(bf16)
            if b < si:
                down_out[c, p, b] = value
                down_sum(c, b, p).start()
            elif c == 0:
                vg[p] = value
                send_vg(p)
            else:
                kg_ref[:, lanes(p)] = value

    def pass_up(si, p, total):
        for j in range(n - si):
            value = total[rows * j : rows * (j + 1)]
            if si > 0:
                up_sum(j, p).wait_recv()
                value = value + up_in[p, j].astype(f32)
            value = value.astype(bf16)
            if j < last - si:
                up_out[p, j] = value
                up_sum(j, p).start()
            else:
                qg_ref[:, lanes(half + p)] = value

    def each(body, begin=0, end=half):
        def step(p, carry):
            body(p)
            return carry

        lax.fori_loop(begin, end, step, 0)

    def relay_up(si, a, t, p):
        if si - t >= 0 and si < last:
            up_arrive(a, si - t, p)
            up(si, a, si - t, p).start()

    def relay_down(si, a, t, p):
        if si + t <= last and si > 0:
            down_arrive(a, si + t, p)
            down(si, a, si + t, p).start()

    def send_own(si, upward, begin, end):
        for p in range(begin, end):
            (up if upward else down)(si, 1, si, p).start()

    def relay(si, a, t):
        for p in range(half):
            relay_up(si, a, t, p)
            relay_down(si, a, t, p)

    def relay_first(si):
        if si in (0, last):
            return
        upper = 2 * si >= n
        relay(si, 0, 1)
        send_own(si, not upper, 0, half)
        early = 0 if upper else half // 2
        send_own(si, upper, 0, early)
        for t in range(2, n):
            relay(si, 0, t)
        send_own(si, upper, early, half)

    def w_relay_up(si, t):
        if si - t >= 0:
            hop(si, si - t, True).wait_recv()
            if si < last:
                hop(si, si - t, True).start()
            w_start(si - t)

    def w_relay_down(si, t):
        if si + t <= last:
            hop(si, si + t, False).wait_recv()
            if si > 0:
                hop(si, si + t, False).start()
            w_start(si + t)

    def w_relay(si, t):
        w_relay_up(si, t)
        w_relay_down(si, t)

    def w_blocks(si, t):
        return [b for b in (si - t, si + t) if 0 <= b <= last]

    def first(si):
        columns, query_columns = rows * (si + 1), rows * (n - si)
        others = [u for u in range(n) if u != si]
        for p in range(half):
            if si < last:
                up(si, 0, si, p).start()
            if si > 0:
                down(si, 0, si, p).start()
        for u in others:
            gate_copy(si, u).start()
        if si == 0:
            send_own(si, True, 0, half)
            hop(si, si, True).start()
        if si == last:
            send_own(si, False, 0, half)
            hop(si, si, False).start()
        for name in x_start:
            x_copy(name).start()
        w_start(si, True)

        for p in range(half):
            for a, ref in enumerate((k_ref, v_ref)):
                kv_in[a, p, si] = ref[:, lanes(p)]
            for a, ref in enumerate((q_ref, g_ref)):
                qg_in[a, p, last - si] = ref[:, lanes(half + p)]
        relay_first(si)

        gate_pad[...] = jnp.zeros_like(gate_pad)
        for which in range(2):
            stats[which, si] = jnp.zeros(stats.shape[2:], f32)
        peaks[...] = jnp.zeros_like(peaks)
        held = gate_ref.shape[0]
        length = rows * n
        gate_pad[held * si : held * si + held, :length] = gate_ref[...]
        arrived("gate", gate_all.at[:last])
        for u in others:
            gate_pad[held * u : held * u + held, :length] = gate_all[u]
        turned = gate_pad[...].T
        gate_t[...] = turned
        back = [turned[rows * b : rows * (b + 1)] for b in reversed(range(n))]
        gate_rev[...] = jnp.concatenate(back + [turned[length:]], axis=0).T

        def queries_step(p):
            relay_up(si, 1, 1, p)
            if si == last:
                for b in range(si):
                    up_arrive(0, b, p)
            total = softmax_queries(si, p)
            if si == last:
                pass_down(si, 0, p, total)
            else:
                down_acc[0, p, : si + 1] = total.reshape(si + 1, rows, LANES)

        def keys_step(p):
            if 2 * si >= n:
                relay_down(si, 1, 1, p)
            if si == 0:
                for b in range(1, n):
                    down_arrive(0, b, p)
            softmax_keys(si, p)

        def gradient_step(p):
            if si == last:
                for b in range(si):
                    up_arrive(1, b, p)
            total = gradient_queries(si, p)
            if si == last:
                pass_down(si, 1, p, total)
            else:
                down_acc[1, p, : si + 1] = total.reshape(si + 1, rows, LANES)

        def do_keys():
            each(keys_step)
            for u in others:
                stat_copy(0, si, u).start()

        if si == 0:
            each(queries_step)
            do_keys()
            each(gradient_step)
        elif 2 * si < n:
            each(queries_step)
            for p in range(half // 2):
                relay_down(si, 1, 1, p)
            do_keys()
            for p in range(half // 2, half):
                relay_down(si, 1, 1, p)
            hop(si, si, True).start()
        elif si < last:
            do_keys()
            hop(si, si, False).start()
            each(queries_step)
        else:
            do_keys()
            each(queries_step)
        x_middle()
        for t in range(2, n):
            relay(si, 1, t)
        if 0 < si < last:
            if 2 * si < n:
                w_relay_up(si, 1)
            else:
                hop(si, si, True).start()
        x_all[d] = in_ref[...]
        w_all[d, si] = w_ref[...]

        def value_step(p):
            if si == 0:
                for b in range(1, n):
                    down_arrive(1, b, p)
            value_keys(si, p)

        def do_values():
            for u in others:
                stat_copy(0, u, si).wait_recv()
            join_peaks(si)
            each(value_step)
            for u in others:
                stat_copy(1, si, u).start()

        def value_sums(begin=0, end=half):
            each(lambda p: pass_down(si, 0, p, down_acc[0, p, : si + 1].reshape(columns, LANES)), begin, end)

        def key_gradient_step(p):
            total = gradient_keys(si, p)
            if si == 0:
                pass_up(si, p, total)
            else:
                up_acc[p, : n - si] = total.reshape(n - si, rows, LANES)

        def do_key_gradients():
            for u in others:
                stat_copy(1, u, si).wait_recv()
            join_terms(si)
            each(key_gradient_step)

        if si == 0:
            do_values()
            x_over()
            w_middle(si)
            do_key_gradients()
            w_relay(si, 1)
            x_last()
            value_sums()
            w_relay(si, 2)
        elif si == last:
            do_values()
            x_over()
            w_middle(si)
            each(gradient_step)
            w_relay(si, 1)
            x_last()
            do_key_gradients()
            w_relay(si, 2)
        elif 2 * si < n:
            do_values()
            hop(si, si, False).start()
            x_over()
            w_middle(si)
            each(gradient_step)
            value_sums()
            w_relay_down(si, 1)
            x_last()
            do_key_gradients()
            w_relay(si, 2)
            chain_first(si, 0, half // 2)
        else:
            value_sums(0, half // 2)
            do_values()
            value_sums(half // 2, half - 1)
            each(gradient_step, 0, half // 2)
            value_sums(half - 1, half)
            w_relay_down(si, 1)
            x_over()
            w_middle(si)
            w_relay_up(si, 1)
            each(gradient_step, half // 2, half)
            x_last()
            chain_first(si, 0, half // 2)
            do_key_gradients()
            w_relay(si, 2)

    def chain_down(si, begin, end):
        if si < last:
            for p in range(begin, end):
                pass_down(si, 1, p, down_acc[1, p, : si + 1].reshape(rows * (si + 1), LANES))

    def chain_up(si, begin, end):
        if si > 0:
            for p in range(begin, end):
                pass_up(si, p, up_acc[p, : n - si].reshape(rows * (n - si), LANES))

    def chain_first(si, begin, end):
        (chain_up if 2 * si < n else chain_down)(si, begin, end)

    def chain_other(si, begin, end):
        (chain_down if 2 * si < n else chain_up)(si, begin, end)

    def chain_rest(si):
        if si in (0, last):
            chain_other(si, 0, half)

    def fourth(si):
        w_relay(si, 3)
        w_last(si)

    def fifth(si):
        for j in w_blocks(si, 1):
            w_middle(j)

    def sixth(si):
        for j in w_blocks(si, 2):
            w_middle(j)
        for j in w_blocks(si, 1):
            w_last(j)
        for j in w_blocks(si, 3):
            w_middle(j)

    def seventh(si):
        for t in (2, 3):
            for j in w_blocks(si, t):
                w_last(j)

    def finish(si):
        if si < last:
            sent("up", kv_in.at[:, :, : si + 1])
            sent("up sum", up_out.at[:, : last - si])
            sent(("hop", True), w_all.at[0, : si + 1])
        if si > 0:
            sent("down", qg_in.at[:, :, : n - si])
            sent("down sum", down_out.at[:, :, :si])
            sent(("hop", False), w_all.at[0, : n - si])
        width = sum(stat_width(si, u) for u in range(n) if u != si)
        count = next(c for c in range(1, n + 1) if width % (c * LANES) == 0 and width // c <= stats.shape[3])
        for which in range(2):
            sent(("stat", which), stats.at[0, :count, :, : width // count])

    def by_device(body):
        for si in range(n):
            @pl.when(s == si)
            def _():
                body(si)

    barrier = pltpu.get_barrier_semaphore()
    for r in range(1, n):
        pl.semaphore_signal(barrier, inc=1, device_id={"sp": (s + r) % n, "dp": d}, device_id_type=MESH)
    for step in range(1, 8):
        pl.semaphore_signal(barrier, inc=1, device_id={"sp": s, "dp": near(step)}, device_id_type=MESH)
    pl.semaphore_wait(barrier, n - 1 + 7)
    for copy in fetched:
        copy.wait()

    by_device(first)

    arrived(("x", "x over"), x_all.at[:4])
    arrived("vg", vg_seq.at[:7])

    def weight_part(j):
        columns = pl.ds(pl.multiple_of(j * block, LANES), block)
        total = None
        for i in range(8):
            total = plus(total, dot(vg_seq[i], x_all[i, :, columns], BY_ROWS))
        return total

    side = s // 2
    mate = s + 1 - 2 * (s % 2)
    outer = (s == 0) | (s == last)
    inner = (s > 0) & (s < last)
    outermost, nearest = (1 - side) * last, 2 - side

    def part_copy(j, slot, to):
        return remote(part.at[j], part_in.at[slot], "part", sem("part", 4) + slot, to, d)

    def give(j, k, slot):
        part[j] = sum_ref[k].astype(bf16)
        part_copy(j, slot, mate).start()

    sum_ref[0] = weight_part(jnp.where(outer, outermost, mate))
    pl.when(outer)(lambda: give(outermost, 0, 0))
    pl.when(inner)(lambda: give(mate, 0, 2))
    sum_ref[1] = weight_part(jnp.where(outer, nearest, outermost))
    pl.when(outer)(lambda: give(nearest, 1, 1))
    pl.when(s == 0)(lambda: fourth(0))
    sum_ref[2] = weight_part(jnp.where(outer, mate, nearest))
    pl.when(outer)(lambda: give(mate, 2, 2))
    sum_ref[3] = weight_part(s)
    by_device(lambda si: si > 0 and fourth(si))
    by_device(lambda si: chain_first(si, half // 2, half))
    by_device(fifth)

    def pass_part(k, j):
        part_copy(j, k, j).wait_recv()
        part[j] = (sum_ref[k + 1] + part_in[k].astype(f32)).astype(bf16)
        part_copy(j, 3, j).start()

    def input_part(j):
        remote(w_all.at[:4, j], w_all.at[:4, j], "w", sem("w over", n) + j, s, partner).wait_recv()
        vg_rows = jnp.concatenate([vg[i] for i in range(8)], axis=1)
        w_rows = jnp.concatenate([w_all[i, j] for i in range(8)], axis=1)
        columns = pl.ds(pl.multiple_of(j * block, LANES), block)
        ig_ref[:, columns] = dot(vg_rows, w_rows, BY_LANES).astype(bf16)

    input_part(s)
    for step, j in enumerate((outermost, nearest)):
        by_device(lambda si: 0 < si < last and chain_other(si, step * half // 2, (step + 1) * half // 2))
        pl.when(inner)(lambda: pass_part(step, j))

    by_device(sixth)
    input_part(mate)
    by_device(seventh)
    input_part(nearest)
    input_part(outermost)
    by_device(chain_rest)

    by_device(finish)
    sent("gate", gate_all.at[:last])
    sent("vg", vg_seq.at[:7])
    sent("x", x_all.at[:7])
    sent("w", w_all.at[:7])

    for slot in (2, 3):
        part_copy(s, slot, mate).wait_recv()
    total = sum_ref[3] + part_in[2].astype(f32) + part_in[3].astype(f32)
    wg_ref[...] = total.T
    sent("part", part.at[:3])


def put_out(*refs):
    sems = refs[-1]
    copies = [pltpu.make_async_copy(refs[i], refs[4 + i], sems.at[i]) for i in range(4)]
    for copy in copies:
        copy.start()
    for copy in copies:
        copy.wait()


def fused(mesh, inputs, query, key, value, cotangent, gate, weight):
    n = mesh.shape["sp"]
    rows, width = query.shape[1:]
    model = inputs.shape[2]
    half = width // LANES // 2
    length = n * rows
    wide = padded(length)
    bf16, f32 = jnp.bfloat16, jnp.float32
    copies = 7 * (n - 1) * half + 8 * n + 12
    vmem = pl.BlockSpec(memory_space=pltpu.VMEM)
    hbm = pl.BlockSpec(memory_space=pl.ANY)
    results = (
        jax.ShapeDtypeStruct((rows, width), bf16),
        jax.ShapeDtypeStruct((rows, width), bf16),
        jax.ShapeDtypeStruct((rows, model), bf16),
        jax.ShapeDtypeStruct((model // n, LANES), f32),
    )
    outs = pl.pallas_call(
        functools.partial(kernel, n, half),
        out_shape=tuple(pltpu.VMEM(x.shape, x.dtype) for x in results),
        in_specs=[hbm] * 5 + [vmem, hbm],
        out_specs=(vmem,) * 4,
        scratch_shapes=[
            pltpu.VMEM((rows, model), bf16),
            *[pltpu.VMEM((rows, width), bf16)] * 4,
            pltpu.VMEM((model // n, LANES), bf16),
            *[pltpu.VMEM((2, half, n, rows, LANES), bf16)] * 2,
            *[pltpu.VMEM((2, half, n - 1, rows, LANES), bf16)] * 2,
            *[pltpu.VMEM((half, n - 1, rows, LANES), bf16)] * 2,
            pltpu.VMEM((2, half, n, rows, LANES), f32),
            pltpu.VMEM((half, n, rows, LANES), f32),
            pltpu.VMEM((8, rows, LANES), bf16),
            pltpu.VMEM((8, rows, LANES), bf16),
            pltpu.VMEM((8, rows, model), bf16),
            pltpu.VMEM((8, n, model // n, LANES), bf16),
            pltpu.VMEM((n, LANES, model // n), bf16),
            pltpu.VMEM((4, LANES, model // n), bf16),
            pltpu.VMEM((4, LANES, model // n), f32),
            pltpu.VMEM((n, gate.shape[1], length), f32),
            pltpu.VMEM((LANES, wide), f32),
            pltpu.VMEM((wide, LANES), f32),
            pltpu.VMEM((LANES, wide), f32),
            *[pltpu.VMEM((2 * half, rows, length), f32)] * 3,
            *[pltpu.VMEM((2 * half, wide), f32)] * 3,
            pltpu.VMEM((2, n, 2 * half, wide), f32),
            pltpu.SemaphoreType.DMA((6,)),
            pltpu.SemaphoreType.DMA((13,)),
            pltpu.SemaphoreType.DMA((copies,)),
        ],
        compiler_params=pltpu.CompilerParams(
            collective_id=0, has_side_effects=True, vmem_limit_bytes=60 * 2**20
        ),
    )(inputs[0], query[0], key[0], value[0], cotangent[0], gate[0], weight)
    query_grad, key_grad, input_grad, weight_grad = pl.pallas_call(
        put_out,
        out_shape=results,
        in_specs=[vmem] * 4,
        out_specs=(hbm,) * 4,
        scratch_shapes=[pltpu.SemaphoreType.DMA((4,))],
        compiler_params=pltpu.CompilerParams(vmem_limit_bytes=2**20),
    )(*(pltpu.with_memory_space_constraint(x, pltpu.VMEM) for x in outs))
    return (query_grad[None], key_grad[None], input_grad[None], weight_grad)


def solution(mesh):
    in_specs = (
        P("dp", "sp", None),
        P("dp", "sp", None),
        P("dp", "sp", None),
        P("dp", "sp", None),
        P("dp", "sp", None),
        P("dp", "sp", None),
        P("sp", "dp"),
    )
    out_specs = (P("dp", "sp", None), P("dp", "sp", None), P("dp", "sp", None), P("sp", "dp"))
    sp_count, dp_count = mesh.shape["sp"], mesh.shape["dp"]

    def per_device(*arrays):
        if one_kernel_fits(sp_count, dp_count, *arrays):
            return fused(mesh, *arrays)
        return shards(*arrays)

    return jax.shard_map(per_device, mesh=mesh, in_specs=in_specs, out_specs=out_specs, check_vma=False)
```

```python
import functools

import jax
import jax.numpy as jnp
from jax import lax
from jax.experimental import pallas as pl
from jax.experimental.pallas import tpu as pltpu
from jax.sharding import PartitionSpec as P

HEAD_DIM = 64


def attention_backward(query_heads, key_heads, value_heads, grad_heads, prefix):
    length = query_heads.shape[0]
    score_scale = HEAD_DIM ** (-0.5)
    block_count = max(1, length // 512)
    block_rows = length // block_count
    key_accum = jnp.zeros(key_heads.shape, jnp.float32)
    value_accum = jnp.zeros(key_heads.shape, jnp.float32)
    query_parts = []
    for block_index in range(block_count):
        first_row = block_index * block_rows
        last_row = first_row + block_rows
        query_rows = query_heads[first_row:last_row]
        key_rows = key_heads[:last_row]
        grad_rows = grad_heads[first_row:last_row]
        scores = (
            jnp.einsum("qhd,khd->hqk", query_rows, key_rows, preferred_element_type=jnp.float32)
            * score_scale
        )
        scores = scores + prefix[:, first_row:last_row, None] - prefix[:, None, :last_row]
        causal = jnp.arange(last_row)[None, :] <= (first_row + jnp.arange(block_rows))[:, None]
        scores = jnp.where(causal[None], scores, -jnp.inf)
        row_peak = jnp.max(scores, axis=-1, keepdims=True)
        raised_scores = jnp.exp(scores - row_peak)
        softmax_rows = raised_scores / jnp.sum(raised_scores, axis=-1, keepdims=True)
        softmax_low = softmax_rows.astype(jnp.bfloat16)
        value_accum = value_accum.at[:last_row].add(
            jnp.einsum("hqk,qhd->khd", softmax_low, grad_rows, preferred_element_type=jnp.float32)
        )
        softmax_grad = jnp.einsum(
            "qhd,khd->hqk", grad_rows, value_heads[:last_row], preferred_element_type=jnp.float32
        )
        row_term = jnp.sum(softmax_rows * softmax_grad, axis=-1, keepdims=True)
        score_low = (softmax_rows * (softmax_grad - row_term)).astype(jnp.bfloat16)
        query_parts.append(
            (
                jnp.einsum("hqk,khd->qhd", score_low, key_rows, preferred_element_type=jnp.float32)
                * score_scale
            ).astype(jnp.bfloat16)
        )
        key_accum = key_accum.at[:last_row].add(
            jnp.einsum("hqk,qhd->khd", score_low, query_rows, preferred_element_type=jnp.float32)
        )
    query_grad = jnp.concatenate(query_parts, axis=0)
    key_grad = (key_accum * score_scale).astype(jnp.bfloat16)
    return (query_grad, key_grad, value_accum.astype(jnp.bfloat16))


def shards(inputs, query_vectors, key_vectors, value_vectors, cotangent, gate_prefix, value_weight):
    query_seq, key_seq, value_seq, grad_seq, input_cols = (
        lax.all_to_all(query_vectors[0], "sp", split_axis=1, concat_axis=0, tiled=True),
        lax.all_to_all(key_vectors[0], "sp", split_axis=1, concat_axis=0, tiled=True),
        lax.all_to_all(value_vectors[0], "sp", split_axis=1, concat_axis=0, tiled=True),
        lax.all_to_all(cotangent[0], "sp", split_axis=1, concat_axis=0, tiled=True),
        lax.all_to_all(inputs[0], "sp", split_axis=1, concat_axis=0, tiled=True),
    )
    length = query_seq.shape[0]
    local_width = query_seq.shape[1]
    head_shape = (length, local_width // HEAD_DIM, HEAD_DIM)
    query_heads, key_heads, value_heads = attention_backward(
        query_seq.reshape(head_shape),
        key_seq.reshape(head_shape),
        value_seq.reshape(head_shape),
        grad_seq.reshape(head_shape),
        gate_prefix[0],
    )
    query_flat = query_heads.reshape(length, local_width)
    key_flat = key_heads.reshape(length, local_width)
    value_flat = value_heads.reshape(length, local_width)
    value_all = lax.all_gather(value_flat, "sp", axis=1, tiled=True)
    weight_block = lax.all_gather(value_weight, "dp", axis=1, tiled=True)
    weight_rows = lax.psum_scatter(
        lax.dot_general(
            value_all, input_cols, (((0,), (0,)), ((), ())), preferred_element_type=jnp.float32
        ).astype(jnp.bfloat16),
        "dp",
        scatter_dimension=0,
        tiled=True,
    ).astype(jnp.float32)
    weight_grad = weight_rows.T
    query_back, key_back = (
        lax.all_to_all(query_flat, "sp", split_axis=0, concat_axis=1, tiled=True),
        lax.all_to_all(key_flat, "sp", split_axis=0, concat_axis=1, tiled=True),
    )
    column_grad = lax.dot_general(
        value_all, weight_block, (((1,), (1,)), ((), ())), preferred_element_type=jnp.float32
    ).astype(jnp.bfloat16)
    input_grad = lax.all_to_all(column_grad, "sp", split_axis=0, concat_axis=1, tiled=True)
    return (query_back[None], key_back[None], input_grad[None], weight_grad)


LANES = 128
MESH = pl.DeviceIdType.MESH


def one_kernel_fits(sp_count, dp_count, inputs, query, key, value, cotangent, gate, weight):
    rows, width = query.shape[1:]
    model = inputs.shape[2]
    return (
        dp_count == 8
        and width == dp_count * LANES
        and width % (sp_count * LANES) == 0
        and gate.shape[1] * sp_count * HEAD_DIM == width
        and gate.shape[2] == rows * sp_count
        and LANES == 2 * HEAD_DIM
        and rows % 8 == 0
        and model % (sp_count * LANES) == 0
        and model % (2 * LANES) == 0
        and sp_count == 4
        and rows * sp_count <= 1024
        and (dp_count * rows + width) * model <= 3 * 2**21
    )


dot = functools.partial(lax.dot_general, preferred_element_type=jnp.float32)
BY_LANES = (((1,), (1,)), ((), ()))
BY_ROWS = (((0,), (0,)), ((), ()))
PLAIN = (((1,), (0,)), ((), ()))
LOWEST = -1e30


def own_lanes(head, *arrays):
    lane = lax.broadcasted_iota(jnp.int32, arrays[0].shape, 1)
    own = (lane < HEAD_DIM) if head == 0 else (lane >= HEAD_DIM)
    return [jnp.where(own, x, 0.0).astype(jnp.bfloat16) for x in arrays]


def lanes(p):
    return pl.ds(p * LANES if isinstance(p, int) else pl.multiple_of(p * LANES, LANES), LANES)


def padded(columns):
    return -(-columns // LANES) * LANES


def plus(total, term):
    return term if total is None else total + term


def causal(scores, rows, keys_first):
    columns = scores.shape[1]
    start = columns - rows
    low = start // LANES * LANES
    tail = scores[:, low:]
    row = lax.broadcasted_iota(jnp.int32, tail.shape, 0)
    column = lax.broadcasted_iota(jnp.int32, tail.shape, 1) + (low - start)
    kept = ((column >= row) | (column < 0)) if keys_first else (column <= row)
    tail = jnp.where(kept, tail, -jnp.inf)
    return jnp.concatenate([scores[:, :low], tail], axis=1) if low else tail


def kernel(
    n, half, in_hbm, q_hbm, k_hbm, v_hbm, g_hbm, gate_ref, w_hbm,
    qg_ref, kg_ref, ig_ref, wg_ref,
    in_ref, q_ref, k_ref, v_ref, g_ref, w_ref,
    kv_in, qg_in, down_in, down_out, up_in, up_out, down_acc, up_acc,
    vg, vg_seq, x_all, w_all, part, part_in, sum_ref,
    gate_all, gate_pad, gate_t, gate_rev, soft, raised, value_dot,
    peaks, factors, row_terms, stats,
    local_sems, send_sems, recv_sems,
):
    s = lax.axis_index("sp")
    d = lax.axis_index("dp")
    core, x, y = d % 2, (d // 2) % 2, d // 4
    rows, model = in_ref.shape
    last = n - 1
    low, high = pl.ds(0, model // 2), pl.ds(model // 2, model // 2)
    block = model // n
    scale = HEAD_DIM ** (-0.5)
    f32, bf16 = jnp.float32, jnp.bfloat16

    fetched = [
        pltpu.make_async_copy(src, dst, local_sems.at[i])
        for i, (src, dst) in enumerate(
            ((k_hbm, k_ref), (q_hbm, q_ref), (in_hbm, in_ref), (w_hbm, w_ref), (v_hbm, v_ref), (g_hbm, g_ref))
        )
    ]
    for copy in fetched:
        copy.start()

    def near(step):
        return (
            d
            + (step % 2) * (1 - 2 * core)
            + ((step // 2) % 2) * (2 - 4 * x)
            + (step // 4) * (4 - 8 * y)
        )

    partner, x_near, y_near, corner = near(1), near(2), near(4), near(6)

    ids = {}
    used = [0]

    def sem(key, count=1):
        if key not in ids:
            ids[key] = used[0]
            used[0] += count
            assert used[0] <= recv_sems.shape[0], (key, used, recv_sems.shape)
        return ids[key]

    sent_ids = {}

    def remote(src, dst, kind, recv_id, to_sp, to_dp):
        send_id = sent_ids.setdefault(kind, len(sent_ids))
        assert send_id < send_sems.shape[0]
        return pltpu.make_async_remote_copy(
            src_ref=src,
            dst_ref=dst,
            send_sem=send_sems.at[send_id],
            recv_sem=recv_sems.at[recv_id],
            device_id={"sp": to_sp, "dp": to_dp},
            device_id_type=MESH,
        )

    def sent(kind, ref):
        remote(ref, ref, kind, 0, s, partner).wait_send()

    def arrived(name, ref):
        remote(ref, ref, "up", sem(name), s, partner).wait_recv()

    def up(si, a, b, p):
        src = (k_ref, v_ref)[a].at[:, lanes(p)] if b == si else kv_in.at[a, p, b]
        i = sem(("up", a, b), half) + p
        return remote(src, kv_in.at[a, p, b], "up", i, s + 1, d)

    def up_arrive(a, b, p):
        i = sem(("up", a, b), half) + p
        remote(kv_in.at[a, p, b], kv_in.at[a, p, b], "up", i, (s + 1) % n, d).wait_recv()

    def down(si, a, b, p):
        src = (q_ref, g_ref)[a].at[:, lanes(half + p)] if b == si else qg_in.at[a, p, last - b]
        i = sem(("down", a, b), half) + p
        return remote(src, qg_in.at[a, p, last - b], "down", i, s - 1, d)

    def down_arrive(a, b, p):
        i = sem(("down", a, b), half) + p
        remote(qg_in.at[a, p, last - b], qg_in.at[a, p, last - b], "down", i, (s + 1) % n, d).wait_recv()

    def down_sum(c, b, p):
        i = sem(("down sum", c, b * (1 - c)), half) + p
        return remote(down_out.at[c, p, b], down_in.at[c, p, b], "down sum", i, (s + n - 1) % n, d)

    def up_sum(j, p):
        i = sem("up sum", half) + p
        return remote(up_out.at[p, j], up_in.at[p, j], "up sum", i, (s + 1) % n, d)

    def gate_copy(sender, to):
        return remote(gate_ref, gate_all.at[sender], "gate", sem("gate"), to, d)

    def stat_width(a, b):
        return padded(rows * (n - max(a, b)))

    def stat_copy(which, sender, to):
        i = sem(("stat", which), n)
        piece = stats.at[which, sender, :, pl.ds(0, stat_width(sender, to))]
        return remote(piece, piece, ("stat", which), i + sender, to, d)

    def hop(si, b, upward):
        src = w_ref if b == si else w_all.at[d, b]
        i = sem(("hop", upward), n) + b
        return remote(src, w_all.at[d, b], ("hop", upward), i, (s + 1) % n if upward else (s + n - 1) % n, d)

    def vg_copy(p):
        return remote(vg.at[p], vg_seq.at[d], "vg", sem("vg"), s, p)

    def send_vg(p):
        @pl.when(d != p)
        def _():
            vg_copy(p).start()

        @pl.when(d == p)
        def _():
            vg_seq[p] = vg[p]

    def x_copy(name):
        src, dst, to = {
            "x low": (in_ref.at[:, low], x_all.at[d, :, low], x_near),
            "x high": (in_ref.at[:, high], x_all.at[d, :, high], x_near),
            "y high": (in_ref.at[:, high], x_all.at[d, :, high], y_near),
            "y low": (in_ref.at[:, low], x_all.at[d, :, low], y_near),
            "own": (in_ref, x_all.at[d], partner),
            "on y": (x_all.at[x_near, :, low],) * 2 + (y_near,),
            "on x": (x_all.at[y_near, :, high],) * 2 + (x_near,),
            "x over": (x_all.at[x_near],) * 2 + (partner,),
            "y over": (x_all.at[y_near],) * 2 + (partner,),
            "corner over": (x_all.at[corner],) * 2 + (partner,),
        }[name]
        key = "x on" if name[:2] == "on" else "x over" if name[-4:] == "over" or name == "own" else name
        return remote(src, dst, "x", sem(("x", key)), s, to)

    x_start = ("x low", "y high", "x high", "y low", "own")

    def x_middle():
        x_copy("x low").wait_recv()
        x_copy("on y").start()
        x_copy("y high").wait_recv()
        x_copy("on x").start()

    def x_over():
        x_copy("x high").wait_recv()
        x_copy("x over").start()
        x_copy("y low").wait_recv()
        x_copy("y over").start()

    def x_last():
        arrived(("x", "x on"), x_all.at[corner])
        x_copy("corner over").start()

    w_lower, w_upper = pl.ds(0, block // 2), pl.ds(block // 2, block // 2)

    def w_copy(name, j, own=False):
        first = w_ref if own else w_all.at[d, j]
        src, dst, to = {
            "x": (first, w_all.at[d, j], x_near),
            "y": (first, w_all.at[d, j], y_near),
            "own": (first, w_all.at[d, j], partner),
            "on y": (w_all.at[x_near, j, w_lower],) * 2 + (y_near,),
            "on x": (w_all.at[y_near, j, w_upper],) * 2 + (x_near,),
            "x over": (w_all.at[x_near, j],) * 2 + (partner,),
            "y over": (w_all.at[y_near, j],) * 2 + (partner,),
            "corner over": (w_all.at[corner, j],) * 2 + (partner,),
        }[name]
        if name[-4:] == "over" or name == "own":
            return remote(src, dst, "w", sem("w over", n) + j, s, to)
        key = ("on", j) if name[:2] == "on" else (name, j)
        return remote(src, dst, "w", sem(("w", key)), s, to)

    def w_start(j, own=False):
        for name in ("x", "y", "own"):
            w_copy(name, j, own).start()

    def w_middle(j):
        w_copy("x", j).wait_recv()
        w_copy("on y", j).start()
        w_copy("y", j).wait_recv()
        w_copy("on x", j).start()
        w_copy("x over", j).start()
        w_copy("y over", j).start()

    def w_last(j):
        arrived(("w", ("on", j)), w_all.at[corner, j])
        w_copy("corner over", j).start()

    def wide(buffer, a, p, count):
        return buffer[a, p, :count].astype(f32).reshape(count * rows, LANES)

    def own32(ref, p):
        return ref[:, lanes(p)].astype(f32)

    def gate_column(si, head):
        own = gate_t[rows * si : rows * si + rows]
        lane = lax.broadcasted_iota(jnp.int32, own.shape, 1)
        return jnp.sum(jnp.where(lane == head, own, 0.0), axis=1, keepdims=True)

    def softmax_queries(si, p):
        columns = rows * (si + 1)
        q32, g32 = own32(q_ref, p), own32(g_ref, p)
        keys = wide(kv_in, 0, p, si + 1).astype(bf16)
        total = None
        for h in range(2):
            head = 2 * p + h
            q_own, g_own = own_lanes(h, q32, g32)
            scores = dot(q_own, keys, BY_LANES) * scale
            scores = scores + gate_column(si, head) - gate_pad[pl.ds(head, 1), :columns]
            scores = causal(scores, rows, False)
            peak = jnp.max(scores, axis=1, keepdims=True)
            up_scores = jnp.exp(scores - peak)
            part_soft = up_scores * (1.0 / jnp.sum(up_scores, axis=1, keepdims=True))
            soft[head, :, :columns] = part_soft
            total = plus(total, dot(part_soft.astype(bf16), g_own, BY_ROWS))
        return total

    def gradient_queries(si, p):
        columns = rows * (si + 1)
        q32, g32 = own32(q_ref, p), own32(g_ref, p)
        keys32 = wide(kv_in, 0, p, si + 1)
        values = wide(kv_in, 1, p, si + 1).astype(bf16)
        dq = dk = None
        for h in range(2):
            q_own, g_own = own_lanes(h, q32, g32)
            (k_own,) = own_lanes(h, keys32)
            part_soft = soft[2 * p + h, :, :columns]
            soft_grad = dot(g_own, values, BY_LANES)
            row_term = jnp.sum(part_soft * soft_grad, axis=1, keepdims=True)
            score_low = (part_soft * (soft_grad - row_term)).astype(bf16)
            dq = plus(dq, dot(score_low, k_own, PLAIN))
            dk = plus(dk, dot(score_low, q_own, BY_ROWS))
        qg_ref[:, lanes(p)] = (dq * scale).astype(bf16)
        return dk * scale

    def softmax_keys(si, p):
        columns = rows * (n - si)
        k32 = own32(k_ref, half + p)
        queries = wide(qg_in, 0, p, n - si).astype(bf16)
        for h in range(2):
            row = 2 * p + h
            head = 2 * half + row
            (k_own,) = own_lanes(h, k32)
            scores = dot(k_own, queries, BY_LANES) * scale
            scores = scores + gate_rev[pl.ds(head, 1), :columns] - gate_column(si, head)
            scores = causal(scores, rows, True)
            peak = jnp.max(scores, axis=0, keepdims=True)
            up_scores = jnp.exp(scores - peak)
            raised[row, :, :columns] = up_scores
            peaks[pl.ds(row, 1), :columns] = peak
            stats[0, si, pl.ds(row, 1), :columns] = peak + jnp.log(
                jnp.sum(up_scores, axis=0, keepdims=True)
            )

    def stat_pieces(si, which, empty):
        width = padded(rows * (n - si))
        pieces = []
        for u in range(n):
            held = stat_width(si, u)
            piece = stats[which, u, :, :held]
            lane = lax.broadcasted_iota(jnp.int32, piece.shape, 1)
            piece = jnp.where(lane < rows * (n - u), piece, empty)
            if held < width:
                rest = jnp.full((piece.shape[0], width - held), empty, f32)
                piece = jnp.concatenate([piece, rest], axis=1)
            pieces.append(piece)
        return pieces, width

    def join_peaks(si):
        pieces, width = stat_pieces(si, 0, LOWEST)
        peak = functools.reduce(jnp.maximum, pieces)
        total = sum(jnp.exp(piece - peak) for piece in pieces)
        factors[:, :width] = jnp.exp(peaks[:, :width] - (peak + jnp.log(total)))

    def join_terms(si):
        pieces, width = stat_pieces(si, 1, 0.0)
        row_terms[:, :width] = sum(pieces)

    def value_keys(si, p):
        columns = rows * (n - si)
        g32 = wide(qg_in, 1, p, n - si)
        g_all = g32.astype(bf16)
        v32 = own32(v_ref, half + p)
        total = None
        for h in range(2):
            row = 2 * p + h
            (g_own,) = own_lanes(h, g32)
            (v_own,) = own_lanes(h, v32)
            part_soft = raised[row, :, :columns] * factors[pl.ds(row, 1), :columns]
            raised[row, :, :columns] = part_soft
            total = plus(total, dot(part_soft.astype(bf16), g_own, PLAIN))
            soft_grad = dot(v_own, g_all, BY_LANES)
            value_dot[row, :, :columns] = soft_grad
            stats[1, si, pl.ds(row, 1), :columns] = jnp.sum(part_soft * soft_grad, axis=0, keepdims=True)
        vg[half + p] = total.astype(bf16)
        send_vg(half + p)

    def gradient_keys(si, p):
        columns = rows * (n - si)
        q32 = wide(qg_in, 0, p, n - si)
        k32 = own32(k_ref, half + p)
        dq = dk = None
        for h in range(2):
            row = 2 * p + h
            (q_own,) = own_lanes(h, q32)
            (k_own,) = own_lanes(h, k32)
            term = row_terms[pl.ds(row, 1), :columns]
            score_low = (raised[row, :, :columns] * (value_dot[row, :, :columns] - term)).astype(bf16)
            dk = plus(dk, dot(score_low, q_own, PLAIN))
            dq = plus(dq, dot(score_low, k_own, BY_ROWS))
        kg_ref[:, lanes(half + p)] = (dk * scale).astype(bf16)
        return dq * scale

    def pass_down(si, c, p, total):
        if c == 1 and si < last:
            held = down_in.at[c, p, : si + 1]
            remote(held, held, "up", sem(("down sum", c, 0), half) + p, s, partner).wait_recv()
        for b in range(si + 1):
            value = total[rows * b : rows * (b + 1)]
            if si < last:
                if c == 0:
                    down_sum(c, b, p).wait_recv()
                value = value + down_in[c, p, b].astype(f32)
            value = value.astype(bf16)
            if b < si:
                down_out[c, p, b] = value
                down_sum(c, b, p).start()
            elif c == 0:
                vg[p] = value
                send_vg(p)
            else:
                kg_ref[:, lanes(p)] = value

    def pass_up(si, p, total):
        if si > 0:
            held = up_in.at[p, : n - si]
            remote(held, held, "up", sem("up sum", half) + p, s, partner).wait_recv()
        for j in range(n - si):
            value = total[rows * j : rows * (j + 1)]
            if si > 0:
                value = value + up_in[p, j].astype(f32)
            value = value.astype(bf16)
            if j < last - si:
                up_out[p, j] = value
                up_sum(j, p).start()
            else:
                qg_ref[:, lanes(half + p)] = value

    def each(body, begin=0, end=half):
        def step(p, carry):
            body(p)
            return carry

        lax.fori_loop(begin, end, step, 0)

    def relay_up(si, a, t, p):
        if si - t >= 0 and si < last:
            up_arrive(a, si - t, p)
            up(si, a, si - t, p).start()

    def relay_down(si, a, t, p):
        if si + t <= last and si > 0:
            down_arrive(a, si + t, p)
            down(si, a, si + t, p).start()

    def send_own(si, upward, begin, end):
        for p in range(begin, end):
            (up if upward else down)(si, 1, si, p).start()

    def relay(si, a, t):
        for p in range(half):
            relay_up(si, a, t, p)
            relay_down(si, a, t, p)

    def relay_first(si):
        if si in (0, last):
            return
        upper = 2 * si >= n
        relay(si, 0, 1)
        send_own(si, not upper, 0, half)
        early = 0 if upper else half // 2
        send_own(si, upper, 0, early)
        for t in range(2, n):
            relay(si, 0, t)
        send_own(si, upper, early, half)

    def w_relay_up(si, t):
        if si - t >= 0:
            hop(si, si - t, True).wait_recv()
            if si < last:
                hop(si, si - t, True).start()
            w_start(si - t)

    def w_relay_down(si, t):
        if si + t <= last:
            hop(si, si + t, False).wait_recv()
            if si > 0:
                hop(si, si + t, False).start()
            w_start(si + t)

    def w_relay(si, t):
        w_relay_up(si, t)
        w_relay_down(si, t)

    def w_blocks(si, t):
        return [b for b in (si - t, si + t) if 0 <= b <= last]

    def first(si):
        columns, query_columns = rows * (si + 1), rows * (n - si)
        others = [u for u in range(n) if u != si]
        for p in range(half):
            if si < last:
                up(si, 0, si, p).start()
            if si > 0:
                down(si, 0, si, p).start()
        for u in others:
            gate_copy(si, u).start()
        if si == 0:
            send_own(si, True, 0, half)
            hop(si, si, True).start()
        if si == last:
            send_own(si, False, 0, half)
            hop(si, si, False).start()
        for name in x_start:
            x_copy(name).start()
        w_start(si, True)

        for p in range(half):
            for a, ref in enumerate((k_ref, v_ref)):
                kv_in[a, p, si] = ref[:, lanes(p)]
            for a, ref in enumerate((q_ref, g_ref)):
                qg_in[a, p, last - si] = ref[:, lanes(half + p)]
        relay_first(si)

        gate_pad[...] = jnp.zeros_like(gate_pad)
        for which in range(2):
            stats[which, si] = jnp.zeros(stats.shape[2:], f32)
        peaks[...] = jnp.zeros_like(peaks)
        held = gate_ref.shape[0]
        length = rows * n
        gate_pad[held * si : held * si + held, :length] = gate_ref[...]
        arrived("gate", gate_all.at[:last])
        for u in others:
            gate_pad[held * u : held * u + held, :length] = gate_all[u]
        turned = gate_pad[...].T
        gate_t[...] = turned
        back = [turned[rows * b : rows * (b + 1)] for b in reversed(range(n))]
        gate_rev[...] = jnp.concatenate(back + [turned[length:]], axis=0).T

        def queries_step(p):
            relay_up(si, 1, 1, p)
            if si == last:
                for b in range(si):
                    up_arrive(0, b, p)
            total = softmax_queries(si, p)
            if si == last:
                pass_down(si, 0, p, total)
            else:
                down_acc[0, p, : si + 1] = total.reshape(si + 1, rows, LANES)

        def keys_step(p):
            if 2 * si >= n:
                relay_down(si, 1, 1, p)
            if si == 0:
                for b in range(1, n):
                    down_arrive(0, b, p)
            softmax_keys(si, p)

        def gradient_step(p):
            if si == last:
                for b in range(si):
                    up_arrive(1, b, p)
            total = gradient_queries(si, p)
            if si == last:
                pass_down(si, 1, p, total)
            else:
                down_acc[1, p, : si + 1] = total.reshape(si + 1, rows, LANES)

        def do_keys():
            each(keys_step)
            for u in others:
                stat_copy(0, si, u).start()

        if si == 0:
            each(queries_step)
            do_keys()
            each(gradient_step)
        elif 2 * si < n:
            each(queries_step)
            for p in range(half // 2):
                relay_down(si, 1, 1, p)
            do_keys()
            for p in range(half // 2, half):
                relay_down(si, 1, 1, p)
            hop(si, si, True).start()
        elif si < last:
            do_keys()
            hop(si, si, False).start()
            each(queries_step)
        else:
            do_keys()
            each(queries_step)
        x_middle()
        for t in range(2, n):
            relay(si, 1, t)
        if 0 < si < last:
            if 2 * si < n:
                w_relay_up(si, 1)
            else:
                hop(si, si, True).start()
        x_all[d] = in_ref[...]
        w_all[d, si] = w_ref[...]
        if si in (0, last):
            w_middle(si)

        def value_step(p):
            if si == 0:
                for b in range(1, n):
                    down_arrive(1, b, p)
            value_keys(si, p)

        def do_values():
            for u in others:
                stat_copy(0, u, si).wait_recv()
            join_peaks(si)
            each(value_step)
            for u in others:
                stat_copy(1, si, u).start()

        def value_sums(begin=0, end=half):
            each(lambda p: pass_down(si, 0, p, down_acc[0, p, : si + 1].reshape(columns, LANES)), begin, end)

        def key_gradient_step(p):
            total = gradient_keys(si, p)
            if si == 0:
                pass_up(si, p, total)
            else:
                up_acc[p, : n - si] = total.reshape(n - si, rows, LANES)

        def do_key_gradients():
            for u in others:
                stat_copy(1, u, si).wait_recv()
            join_terms(si)
            each(key_gradient_step)

        if si == 0:
            do_values()
            x_over()
            do_key_gradients()
            w_relay(si, 1)
            x_last()
            value_sums()
            w_relay(si, 2)
        elif si == last:
            do_values()
            x_over()
            each(gradient_step)
            w_relay(si, 1)
            x_last()
            do_key_gradients()
            w_relay(si, 2)
        elif 2 * si < n:
            do_values()
            hop(si, si, False).start()
            x_over()
            w_middle(si)
            each(gradient_step)
            value_sums()
            w_relay_down(si, 1)
            x_last()
            do_key_gradients()
            w_relay(si, 2)
            chain_first(si, 0, half // 2)
        else:
            value_sums(0, half // 2)
            do_values()
            value_sums(half // 2, half - 1)
            each(gradient_step, 0, half // 2)
            value_sums(half - 1, half)
            w_relay_down(si, 1)
            x_over()
            w_middle(si)
            w_relay_up(si, 1)
            each(gradient_step, half // 2, half)
            x_last()
            chain_first(si, 0, half // 2)
            do_key_gradients()
            w_relay(si, 2)

    def chain_down(si, begin, end):
        if si < last:
            for p in range(begin, end):
                pass_down(si, 1, p, down_acc[1, p, : si + 1].reshape(rows * (si + 1), LANES))

    def chain_up(si, begin, end):
        if si > 0:
            for p in range(begin, end):
                pass_up(si, p, up_acc[p, : n - si].reshape(rows * (n - si), LANES))

    def chain_first(si, begin, end):
        (chain_up if 2 * si < n else chain_down)(si, begin, end)

    def chain_other(si, begin, end):
        (chain_down if 2 * si < n else chain_up)(si, begin, end)

    def chain_rest(si):
        if si in (0, last):
            chain_other(si, 0, half)

    def fourth(si):
        w_relay(si, 3)
        w_last(si)

    def fifth(si):
        for j in w_blocks(si, 1):
            w_middle(j)

    def sixth(si):
        for j in w_blocks(si, 2):
            w_middle(j)
        for j in w_blocks(si, 1):
            w_last(j)
        for j in w_blocks(si, 3):
            w_middle(j)

    def seventh(si):
        for t in (2, 3):
            for j in w_blocks(si, t):
                w_last(j)

    def finish(si):
        if si < last:
            sent("up", kv_in.at[:, :, : si + 1])
            sent("up sum", up_out.at[:, : last - si])
            sent(("hop", True), w_all.at[0, : si + 1])
        if si > 0:
            sent("down", qg_in.at[:, :, : n - si])
            sent("down sum", down_out.at[:, :, :si])
            sent(("hop", False), w_all.at[0, : n - si])
        width = sum(stat_width(si, u) for u in range(n) if u != si)
        count = next(c for c in range(1, n + 1) if width % (c * LANES) == 0 and width // c <= stats.shape[3])
        for which in range(2):
            sent(("stat", which), stats.at[0, :count, :, : width // count])

    def by_device(body):
        for si in range(n):
            @pl.when(s == si)
            def _():
                body(si)

    barrier = pltpu.get_barrier_semaphore()
    for r in range(1, n):
        pl.semaphore_signal(barrier, inc=1, device_id={"sp": (s + r) % n, "dp": d}, device_id_type=MESH)
    for step in range(1, 8):
        pl.semaphore_signal(barrier, inc=1, device_id={"sp": s, "dp": near(step)}, device_id_type=MESH)
    pl.semaphore_wait(barrier, n - 1 + 7)
    for copy in fetched:
        copy.wait()

    by_device(first)

    arrived(("x", "x over"), x_all.at[:4])
    arrived("vg", vg_seq.at[:7])

    def weight_part(j):
        columns = pl.ds(pl.multiple_of(j * block, LANES), block)
        total = None
        for i in range(8):
            total = plus(total, dot(vg_seq[i], x_all[i, :, columns], BY_ROWS))
        return total

    side = s // 2
    mate = s + 1 - 2 * (s % 2)
    outer = (s == 0) | (s == last)
    inner = (s > 0) & (s < last)
    outermost, nearest = (1 - side) * last, 2 - side

    def part_copy(j, slot, to):
        return remote(part.at[j], part_in.at[slot], "part", sem("part", 4) + slot, to, d)

    def give(j, k, slot):
        part[j] = sum_ref[k].astype(bf16)
        part_copy(j, slot, mate).start()

    sum_ref[0] = weight_part(jnp.where(outer, outermost, mate))
    pl.when(outer)(lambda: give(outermost, 0, 0))
    pl.when(inner)(lambda: give(mate, 0, 2))
    sum_ref[1] = weight_part(jnp.where(outer, nearest, outermost))
    pl.when(outer)(lambda: give(nearest, 1, 1))
    pl.when(s == 0)(lambda: fourth(0))
    sum_ref[2] = weight_part(jnp.where(outer, mate, nearest))
    pl.when(outer)(lambda: give(mate, 2, 2))
    sum_ref[3] = weight_part(s)
    by_device(lambda si: si > 0 and fourth(si))
    by_device(lambda si: chain_first(si, half // 2, half))
    by_device(fifth)

    def pass_part(k, j):
        part_copy(j, k, j).wait_recv()
        part[j] = (sum_ref[k + 1] + part_in[k].astype(f32)).astype(bf16)
        part_copy(j, 3, j).start()

    def input_part(j):
        remote(w_all.at[:4, j], w_all.at[:4, j], "w", sem("w over", n) + j, s, partner).wait_recv()
        vg_rows = jnp.concatenate([vg[i] for i in range(8)], axis=1)
        w_rows = jnp.concatenate([w_all[i, j] for i in range(8)], axis=1)
        columns = pl.ds(pl.multiple_of(j * block, LANES), block)
        ig_ref[:, columns] = dot(vg_rows, w_rows, BY_LANES).astype(bf16)

    input_part(s)
    for step, j in enumerate((outermost, nearest)):
        by_device(lambda si: 0 < si < last and chain_other(si, step * half // 2, (step + 1) * half // 2))
        pl.when(inner)(lambda: pass_part(step, j))

    by_device(sixth)
    input_part(mate)
    by_device(seventh)
    input_part(nearest)
    input_part(outermost)
    by_device(chain_rest)

    by_device(finish)
    sent("gate", gate_all.at[:last])
    sent("vg", vg_seq.at[:7])
    sent("x", x_all.at[:7])
    sent("w", w_all.at[:7])

    for slot in (2, 3):
        part_copy(s, slot, mate).wait_recv()
    total = sum_ref[3] + part_in[2].astype(f32) + part_in[3].astype(f32)
    wg_ref[...] = total.T
    sent("part", part.at[:3])


def put_out(*refs):
    sems = refs[-1]
    copies = [pltpu.make_async_copy(refs[i], refs[4 + i], sems.at[i]) for i in range(4)]
    for copy in copies:
        copy.start()
    for copy in copies:
        copy.wait()


def fused(mesh, inputs, query, key, value, cotangent, gate, weight):
    n = mesh.shape["sp"]
    rows, width = query.shape[1:]
    model = inputs.shape[2]
    half = width // LANES // 2
    length = n * rows
    wide = padded(length)
    bf16, f32 = jnp.bfloat16, jnp.float32
    copies = 5 * (n - 1) * half + 2 * half + 8 * n + 12
    vmem = pl.BlockSpec(memory_space=pltpu.VMEM)
    hbm = pl.BlockSpec(memory_space=pl.ANY)
    results = (
        jax.ShapeDtypeStruct((rows, width), bf16),
        jax.ShapeDtypeStruct((rows, width), bf16),
        jax.ShapeDtypeStruct((rows, model), bf16),
        jax.ShapeDtypeStruct((model // n, LANES), f32),
    )
    outs = pl.pallas_call(
        functools.partial(kernel, n, half),
        out_shape=tuple(pltpu.VMEM(x.shape, x.dtype) for x in results),
        in_specs=[hbm] * 5 + [vmem, hbm],
        out_specs=(vmem,) * 4,
        scratch_shapes=[
            pltpu.VMEM((rows, model), bf16),
            *[pltpu.VMEM((rows, width), bf16)] * 4,
            pltpu.VMEM((model // n, LANES), bf16),
            *[pltpu.VMEM((2, half, n, rows, LANES), bf16)] * 2,
            *[pltpu.VMEM((2, half, n - 1, rows, LANES), bf16)] * 2,
            *[pltpu.VMEM((half, n - 1, rows, LANES), bf16)] * 2,
            pltpu.VMEM((2, half, n, rows, LANES), f32),
            pltpu.VMEM((half, n, rows, LANES), f32),
            pltpu.VMEM((8, rows, LANES), bf16),
            pltpu.VMEM((8, rows, LANES), bf16),
            pltpu.VMEM((8, rows, model), bf16),
            pltpu.VMEM((8, n, model // n, LANES), bf16),
            pltpu.VMEM((n, LANES, model // n), bf16),
            pltpu.VMEM((4, LANES, model // n), bf16),
            pltpu.VMEM((4, LANES, model // n), f32),
            pltpu.VMEM((n, gate.shape[1], length), f32),
            pltpu.VMEM((LANES, wide), f32),
            pltpu.VMEM((wide, LANES), f32),
            pltpu.VMEM((LANES, wide), f32),
            *[pltpu.VMEM((2 * half, rows, length), f32)] * 3,
            *[pltpu.VMEM((2 * half, wide), f32)] * 3,
            pltpu.VMEM((2, n, 2 * half, wide), f32),
            pltpu.SemaphoreType.DMA((6,)),
            pltpu.SemaphoreType.DMA((13,)),
            pltpu.SemaphoreType.DMA((copies,)),
        ],
        compiler_params=pltpu.CompilerParams(
            collective_id=0, has_side_effects=True, vmem_limit_bytes=60 * 2**20
        ),
    )(inputs[0], query[0], key[0], value[0], cotangent[0], gate[0], weight)
    query_grad, key_grad, input_grad, weight_grad = pl.pallas_call(
        put_out,
        out_shape=results,
        in_specs=[vmem] * 4,
        out_specs=(hbm,) * 4,
        scratch_shapes=[pltpu.SemaphoreType.DMA((4,))],
        compiler_params=pltpu.CompilerParams(vmem_limit_bytes=2**20),
    )(*(pltpu.with_memory_space_constraint(x, pltpu.VMEM) for x in outs))
    return (query_grad[None], key_grad[None], input_grad[None], weight_grad)


def solution(mesh):
    in_specs = (
        P("dp", "sp", None),
        P("dp", "sp", None),
        P("dp", "sp", None),
        P("dp", "sp", None),
        P("dp", "sp", None),
        P("dp", "sp", None),
        P("sp", "dp"),
    )
    out_specs = (P("dp", "sp", None), P("dp", "sp", None), P("dp", "sp", None), P("sp", "dp"))
    sp_count, dp_count = mesh.shape["sp"], mesh.shape["dp"]

    def per_device(*arrays):
        if one_kernel_fits(sp_count, dp_count, *arrays):
            return fused(mesh, *arrays)
        return shards(*arrays)

    return jax.shard_map(per_device, mesh=mesh, in_specs=in_specs, out_specs=out_specs, check_vma=False)
```
